32 devices in a mesh: sp: 4 (over y, x), tp: 8 (over z, core).
Axes of the slice: x: 2, y: 2, z: 4, core: 2. Of those that a mesh axis runs over, the one named last changes fastest.
Arguments:
- residual: bfloat16 [16384, 2048], P(('sp', 'tp')), may hold values from -6 to 6
- query_values: bfloat16 [16384, 1024], P('sp', 'tp'), may hold values from -6 to 6
- forget_preact: bfloat16 [16384, 1024], P('sp', 'tp'), may hold values from -6 to 6
- value_written: bfloat16 [16384, 1024], P('sp', 'tp'), may hold values from -6 to 6
- output_gate_preact: bfloat16 [16384, 1024], P('sp', 'tp'), may hold values from -6 to 6
- forget_margin: float32 [1024], P('tp'), may hold values from 0 to 0.1
- sudden_decay: float32 [16, 16384], P('tp', 'sp'), may hold values from -0.7 to 0
- head_norm_gain: float32 [64], replicated, may hold values from 0.1 to 1.9
- output_weight_matrix: bfloat16 [1024, 2048], replicated, may hold values from -0.1875 to 0.1875
- mixer_norm_gain: float32 [2048], replicated, may hold values from 0.1 to 1.9
- feedforward_gain: float32 [2048], replicated, may hold values from 0.1 to 1.9
- routed_expert_index: int32 [16384, 2], P(('sp', 'tp')), may hold values from 0 to 3, all different within a row; in each aligned block of 512 rows (0 to 511, 512 to 1023, ...) at most 384 rows name the same one
- routed_expert_weight: float32 [16384, 2], P(('sp', 'tp')), may hold values from 0.2 to 1.5
- expert_gate_matrix: bfloat16 [4, 2048, 1024], P('sp', None, 'tp'), may hold values from -0.125 to 0.125
- expert_up_matrix: bfloat16 [4, 2048, 1024], P('sp', None, 'tp'), may hold values from -0.125 to 0.125
- expert_down_matrix: bfloat16 [4, 2048, 1024], P('sp', None, 'tp'), may hold values from -0.1875 to 0.1875
- common_gate_matrix: bfloat16 [2048, 256], replicated, may hold values from -0.125 to 0.125
- common_up_matrix: bfloat16 [2048, 256], replicated, may hold values from -0.125 to 0.125
- common_down_matrix: bfloat16 [256, 2048], replicated, may hold values from -0.375 to 0.375
- final_norm_gain: float32 [2048], replicated, may hold values from 0.1 to 1.9
Outputs:
- layer_out: bfloat16 [16384, 2048], P(('sp', 'tp'))
The draws below stay inside these ranges and needn't reach their ends.
Inputs may be any that keep to these rules, and one draw needn't show every extreme that they name: `routed_expert_index`: each row names 2 different experts. Among the rows of one device no expert is named by more than 384 rows, and in some devices' rows one expert is named by exactly 384.
All inputs are finite; a program needn't handle non-finite values.
Results may differ from the reference program's by a relative error of at most 0.0075.
Values may be sent and summed in bfloat16 or wider, within the bound.
No kernel may reach another device: no remote copies, remote signals or barrier semaphores. Data moves between devices by JAX's collectives and lax.ppermute only.
A program may use at most 128 MiB of HBM per device.

```python
import math
import jax
import jax.numpy as jnp
import numpy as np
from jax import lax

D = 2048
RECURRENT_HEADS = 16
HEAD_CHANNELS = 64
MIX = 1024
BLOCK = 64
EF = 1024
SF = 256
TOP_K = 2
TOK_DEV = 4096
SEQUENCE_TOKENS = 16384
ROWS = 512
EXPERTS = 4
CAP = 384


def draw_forget_preact(key, part):
    base_key, shift_key = jax.random.split(key)
    spans = SEQUENCE_TOKENS // TOK_DEV
    shifts = jax.random.uniform(shift_key, (spans, 1, 1), jnp.float32, -1.5, 1.5)
    jitter = jnp.clip(jax.random.normal(base_key, (spans, TOK_DEV, MIX), jnp.float32), -4.0, 4.0)
    return (jitter + shifts).reshape(SEQUENCE_TOKENS, MIX).astype(jnp.bfloat16)


def draw_forget_margin(key, part):
    kind_key, slow_key, fast_key = jax.random.split(key, 3)
    quick_share = 0.5
    quick = jax.random.bernoulli(kind_key, quick_share, (RECURRENT_HEADS, 1))
    slower = jnp.exp(jax.random.uniform(slow_key, (RECURRENT_HEADS, HEAD_CHANNELS), jnp.float32, math.log(0.1), 0.0)) / SEQUENCE_TOKENS
    faster = jnp.exp(jax.random.uniform(fast_key, (RECURRENT_HEADS, HEAD_CHANNELS), jnp.float32, math.log(0.03), math.log(0.1)))
    return jnp.where(quick, faster, slower).reshape(MIX).astype(jnp.float32)


def draw_sudden_decay(key, part):
    place_key, depth_key = jax.random.split(key)
    places = jax.random.randint(place_key, (RECURRENT_HEADS, 2), 0, SEQUENCE_TOKENS)
    depths = jnp.log(jax.random.uniform(depth_key, (RECURRENT_HEADS, 2), jnp.float32, 0.5, 0.8))
    positions = jnp.arange(SEQUENCE_TOKENS, dtype=jnp.int32)
    struck = places[:, :, None] == positions[None, None, :]
    return jnp.sum(jnp.where(struck, depths[:, :, None], 0.0), axis=1).astype(jnp.float32)


def block_scale(rng, extent, cuts, low, top_value):
    def one(dim, blocks):
        steps = jax.random.uniform(jax.random.fold_in(jax.random.fold_in(rng, 6), dim), (blocks,), jnp.float32, low / len(cuts), top_value / len(cuts))
        return jnp.repeat(jnp.exp(steps), extent[dim] // blocks).reshape((-1,) + (1,) * (len(extent) - dim - 1))

    factor_of = one(*cuts[0])
    for cut in cuts[1:]:
        factor_of = factor_of * one(*cut)
    return factor_of


def deal_out(rng, own, number, rows, amount, top, reach, lean):
    ranking = jax.random.permutation(rng, amount)
    heavy_load, common = load_shares(amount, rows * top, reach, lean, True), load_shares(amount, rows * top, reach, lean, False)
    places = jnp.arange(amount)

    def named(sizes, rotation):
        used = int((sizes > 0).sum())
        fixed = max(1, used // 4)
        shifted = fixed + (places - fixed + rotation * (used - fixed)) % max(1, amount - fixed)
        return jnp.zeros((amount,), jnp.int32).at[ranking[jnp.where(places < fixed, places, shifted)]].set(jnp.asarray(sizes, jnp.int32))

    sizes = jnp.where(number % 4 == 0, named(heavy_load, number // 4), named(common, number - number // 4 - 1))
    mixed = jax.random.permutation(jax.random.fold_in(own, 3), amount)
    giver, sink = mixed[0:amount // 2 * 2:2], mixed[1:amount // 2 * 2:2]
    slack = jnp.minimum(sizes[giver] - 1, reach - sizes[sink]) // 2
    slack = jnp.where((giver == ranking[0]) | (sink == ranking[0]) | (sizes[sink] == 0), 0, jnp.maximum(slack, 0))
    shifted = jax.random.randint(jax.random.fold_in(own, 4), (amount // 2,), 0, 1 << 20) % (slack + 1)
    sizes = sizes.at[giver].add(-shifted).at[sink].add(shifted)
    members = jnp.searchsorted(jnp.cumsum(sizes), jnp.arange(rows * top), side="right").astype(jnp.int32)
    listing = members.reshape(top, rows).T
    listing = listing[jax.random.permutation(jax.random.fold_in(own, 1), rows)]
    rotation = jax.random.randint(jax.random.fold_in(own, 2), (rows, 1), 0, top)
    return jnp.take_along_axis(listing, (jnp.arange(top)[None, :] + rotation) % top, axis=1)


def load_shares(amount, total, most, skew, full):
    portions = [(1 << 20) // math.isqrt(grade ** skew) + 1 for grade in range(1, amount + 1)]
    largest = most if full else min(most, max(-(-total // amount), total * portions[0] // sum(portions)))
    least = 1 if total - largest >= amount - 1 else 0
    holding, rest = [largest] + [least] * (amount - 1), total - largest - least * (amount - 1)
    while rest > 0:
        movable = [i for i in range(1, amount) if holding[i] < largest] or [i for i in range(1, amount) if holding[i] < most]
        mass, left = sum([portions[i] for i in movable]), rest
        for i in movable:
            addition = min(most - holding[i], max(1, left * portions[i] // mass), rest)
            holding[i] = holding[i] + addition
            rest = rest - addition
    return np.array(holding)


def bell_draw(stream_key, extent, scale, bound, cuts=(), kind=jnp.bfloat16):
    result = jax.random.normal(stream_key, extent, jnp.float32) * scale
    if len(cuts) > 0:
        result = block_scale(stream_key, extent, cuts, -0.22, 0.18) * result
    return jnp.clip(result, min=-bound, max=bound).astype(kind)


def setup_inputs(seed: int = 0) -> dict:
    key_of = jax.random.split(jax.random.key(seed), 21)
    residual = bell_draw(key_of[0], (SEQUENCE_TOKENS, D), 1.0, 6.0, ((0, 32),))
    query_values = bell_draw(key_of[1], (SEQUENCE_TOKENS, MIX), 1.0, 6.0, ((0, 4), (1, 8)))
    forget_preact = draw_forget_preact(jax.random.fold_in(key_of[20], 71), 0)
    value_written = bell_draw(key_of[3], (SEQUENCE_TOKENS, MIX), 1.0, 6.0, ((0, 4), (1, 8)))
    output_gate_preact = bell_draw(key_of[4], (SEQUENCE_TOKENS, MIX), 1.5, 6.0, ((0, 4), (1, 8)))
    forget_margin = draw_forget_margin(jax.random.fold_in(key_of[20], 71), 0)
    sudden_decay = draw_sudden_decay(jax.random.fold_in(key_of[20], 71), 0)
    head_norm_gain = jnp.clip(1.0 + 0.18 * jax.random.normal(key_of[7], (HEAD_CHANNELS,), jnp.float32), 0.1, 1.9)
    output_weight_matrix = bell_draw(key_of[8], (MIX, D), MIX ** -0.5, 0.1875)
    mixer_norm_gain = jnp.clip(1.0 + 0.18 * jax.random.normal(key_of[9], (D,), jnp.float32), 0.1, 1.9)
    feedforward_gain = jnp.clip(1.0 + 0.18 * jax.random.normal(key_of[10], (D,), jnp.float32), 0.1, 1.9)
    routed_expert_index_keys = jax.random.split(jax.random.fold_in(key_of[11], 1), SEQUENCE_TOKENS // ROWS)
    routed_expert_index_turns = jax.random.permutation(jax.random.fold_in(key_of[11], 3), SEQUENCE_TOKENS // ROWS)
    routed_expert_index = jax.vmap(lambda own, number: deal_out(jax.random.fold_in(key_of[11], 2), own, number, ROWS, EXPERTS, TOP_K, CAP, 1))(routed_expert_index_keys, routed_expert_index_turns).reshape((SEQUENCE_TOKENS, TOP_K))
    routed_expert_weight = jnp.clip(0.2 + 1.3 * jax.random.uniform(key_of[12], (SEQUENCE_TOKENS, TOP_K), jnp.float32) ** block_scale(key_of[12], (SEQUENCE_TOKENS, TOP_K), ((0, 32),), -0.2, 0.2), 0.2, 1.5)
    expert_gate_matrix = bell_draw(key_of[13], (EXPERTS, D, EF), D ** -0.5, 0.125, ((0, 4), (2, 8)))
    expert_up_matrix = bell_draw(key_of[14], (EXPERTS, D, EF), D ** -0.5, 0.125, ((0, 4), (2, 8)))
    expert_down_matrix = bell_draw(key_of[15], (EXPERTS, D, EF), EF ** -0.5, 0.1875, ((0, 4), (2, 8)))
    common_gate_matrix = bell_draw(key_of[16], (D, SF), D ** -0.5, 0.125)
    common_up_matrix = bell_draw(key_of[17], (D, SF), D ** -0.5, 0.125)
    common_down_matrix = bell_draw(key_of[18], (SF, D), SF ** -0.5, 0.375)
    final_norm_gain = jnp.clip(1.0 + 0.18 * jax.random.normal(key_of[19], (D,), jnp.float32), 0.1, 1.9)
    return dict(residual=residual, query_values=query_values, forget_preact=forget_preact, value_written=value_written, output_gate_preact=output_gate_preact, forget_margin=forget_margin, sudden_decay=sudden_decay, head_norm_gain=head_norm_gain, output_weight_matrix=output_weight_matrix, mixer_norm_gain=mixer_norm_gain, feedforward_gain=feedforward_gain, routed_expert_index=routed_expert_index, routed_expert_weight=routed_expert_weight, expert_gate_matrix=expert_gate_matrix, expert_up_matrix=expert_up_matrix, expert_down_matrix=expert_down_matrix, common_gate_matrix=common_gate_matrix, common_up_matrix=common_up_matrix, common_down_matrix=common_down_matrix, final_norm_gain=final_norm_gain)


EPS = 1e-06
TOP_PRECISION = lax.Precision.HIGHEST

def rms_scale(values):
    return values * lax.rsqrt(lax.optimization_barrier(jnp.mean(values * values, axis=-1, keepdims=True)) + EPS)

def linear_recurrence(query_values, forget_preact, value_written, forget_margin, sudden_decay):
    blocks_all = SEQUENCE_TOKENS // BLOCK
    key_magnitude = forget_margin * jax.nn.sigmoid(-forget_preact.astype(jnp.float32))
    log_retention = jnp.log1p(-key_magnitude).reshape(SEQUENCE_TOKENS, RECURRENT_HEADS, HEAD_CHANNELS) + sudden_decay.T[:, :, None]

    def block_view(array):
        return array.astype(jnp.float32).reshape(blocks_all, BLOCK, RECURRENT_HEADS, HEAD_CHANNELS).transpose(2, 0, 1, 3)
    queries = block_view(query_values)
    strengths = block_view(key_magnitude)
    values = block_view(value_written)
    running = jnp.cumsum(block_view(log_retention), axis=2)
    middle = running[:, :, BLOCK // 2 - 1:BLOCK // 2]
    closing = running[:, :, -1:]
    scores = jnp.einsum('hncd,hnsd->hncs', queries * jnp.exp(running - middle), strengths * jnp.exp(middle - running), precision=TOP_PRECISION)
    lower = jnp.tril(jnp.ones((BLOCK, BLOCK), bool))
    scores = jnp.where(lower, scores, 0.0)
    inner = jnp.einsum('hncs,hnse->hnce', scores, values, precision=TOP_PRECISION)
    state_per_block = jnp.einsum('hnsd,hnse->hnde', strengths * jnp.exp(closing - running), values, precision=TOP_PRECISION)
    block_keep = jnp.exp(closing[:, :, 0])

    def advance(carry, inputs):
        keep_now, state_now = inputs
        return (keep_now[..., None] * carry + state_now, carry)
    start_state = jnp.zeros((RECURRENT_HEADS, HEAD_CHANNELS, HEAD_CHANNELS), jnp.float32)
    _, earlier = lax.scan(advance, start_state, (jnp.moveaxis(block_keep, 1, 0), jnp.moveaxis(state_per_block, 1, 0)))
    carried = jnp.einsum('hncd,nhde->hnce', queries * jnp.exp(running), earlier, precision=TOP_PRECISION)
    return (inner + carried).transpose(1, 2, 0, 3).reshape(SEQUENCE_TOKENS, RECURRENT_HEADS, HEAD_CHANNELS)

def routed_sum(normed, routed_expert_index, routed_expert_weight, expert_gate_matrix, expert_up_matrix, expert_down_matrix):
    blocks_all = SEQUENCE_TOKENS // ROWS
    ids_blocked = routed_expert_index.reshape(blocks_all, ROWS, TOP_K)
    numbers = jnp.arange(EXPERTS, dtype=jnp.int32)
    hits = lax.optimization_barrier(jnp.sum((ids_blocked[..., None] == numbers).astype(jnp.int32), axis=2))
    before_hits = jnp.cumsum(hits, axis=1) - hits
    slots = jnp.take_along_axis(before_hits, ids_blocked, axis=2)
    block_number = jnp.arange(blocks_all, dtype=jnp.int32)[:, None, None]
    position = ((ids_blocked * blocks_all + block_number) * CAP + slots).astype(jnp.int32)
    owners = jnp.broadcast_to(jnp.arange(SEQUENCE_TOKENS, dtype=jnp.int32).reshape(blocks_all, ROWS, 1), position.shape)
    table = jnp.full((EXPERTS * blocks_all * CAP,), SEQUENCE_TOKENS, jnp.int32)
    table = table.at[position.reshape(-1)].set(owners.reshape(-1)).reshape(EXPERTS, blocks_all * CAP)
    padded = jnp.concatenate([normed, jnp.zeros((1, D), normed.dtype)], axis=0)

    def one_expert(inputs):
        row_index, gate_w, up_w, down_w = inputs
        picked_rows = padded[row_index]
        hidden = (jax.nn.silu(jnp.dot(picked_rows, gate_w, preferred_element_type=jnp.float32)) * jnp.dot(picked_rows, up_w, preferred_element_type=jnp.float32)).astype(jnp.bfloat16)
        produced = lax.dot_general(hidden, down_w, (((1,), (1,)), ((), ())), preferred_element_type=jnp.float32)
        return produced.astype(jnp.bfloat16)
    outputs = lax.map(one_expert, (table, expert_gate_matrix, expert_up_matrix, expert_down_matrix)).reshape(-1, D)
    flat_position = position.reshape(SEQUENCE_TOKENS, TOP_K)
    routed = jnp.zeros((SEQUENCE_TOKENS, D), jnp.float32)
    for route in range(TOP_K):
        routed = routed + routed_expert_weight[:, route:route + 1] * outputs[flat_position[:, route]].astype(jnp.float32)
    return routed

def reference(residual, query_values, forget_preact, value_written, output_gate_preact, forget_margin, sudden_decay, head_norm_gain, output_weight_matrix, mixer_norm_gain, feedforward_gain, routed_expert_index, routed_expert_weight, expert_gate_matrix, expert_up_matrix, expert_down_matrix, common_gate_matrix, common_up_matrix, common_down_matrix, final_norm_gain):
    head_outputs = linear_recurrence(query_values, forget_preact, value_written, forget_margin, sudden_decay)
    opening = jax.nn.sigmoid(output_gate_preact.astype(jnp.float32)).reshape(SEQUENCE_TOKENS, RECURRENT_HEADS, HEAD_CHANNELS)
    mixed = (rms_scale(head_outputs) * head_norm_gain * opening).reshape(SEQUENCE_TOKENS, MIX).astype(jnp.bfloat16)
    projected = jnp.dot(mixed, output_weight_matrix, preferred_element_type=jnp.float32).astype(jnp.bfloat16)
    stream = (residual.astype(jnp.float32) + rms_scale(projected.astype(jnp.float32)) * mixer_norm_gain).astype(jnp.bfloat16)
    normed = (rms_scale(stream.astype(jnp.float32)) * feedforward_gain).astype(jnp.bfloat16)
    shared_hidden = (jax.nn.silu(jnp.dot(normed, common_gate_matrix, preferred_element_type=jnp.float32)) * jnp.dot(normed, common_up_matrix, preferred_element_type=jnp.float32)).astype(jnp.bfloat16)
    shared = jnp.dot(shared_hidden, common_down_matrix, preferred_element_type=jnp.float32)
    routed = routed_sum(normed, routed_expert_index, routed_expert_weight, expert_gate_matrix, expert_up_matrix, expert_down_matrix)
    layer_out = stream.astype(jnp.float32) + rms_scale(shared + routed) * final_norm_gain
    return layer_out.astype(jnp.bfloat16)
```

```python
import functools

import jax
import jax.numpy as jnp
from jax import lax
from jax.experimental import pallas as pl
from jax.experimental.pallas import tpu as pltpu
from jax.sharding import Mesh, PartitionSpec as P

HEAD_CHANNELS = 64
BLOCK = 64
EPS = 1e-06
TOP_PRECISION = lax.Precision.HIGHEST
F32 = jnp.float32
BF16 = jnp.bfloat16

LANES_LANES = (((1,), (1,)), ((), ()))
ROWS_ROWS = (((0,), (0,)), ((), ()))


def rms_scale(values):
    return values * lax.rsqrt(jnp.mean(values * values, axis=-1, keepdims=True) + EPS)


def mm(a, b, dims=(((1,), (0,)), ((), ()))):
    return lax.dot_general(a, b, dims, preferred_element_type=F32)


def scan_kernel(
    q_ref, f_ref, v_ref, margin_ref, sudden_ref, local_ref, lifted_ref, final_ref, state_ref, total_ref
):
    step = pl.program_id(0)
    span, channels = q_ref.shape
    heads = channels // HEAD_CHANNELS

    @pl.when(step == 0)
    def _():
        state_ref[...] = jnp.zeros_like(state_ref)
        total_ref[...] = jnp.zeros_like(total_ref)

    lane = lax.broadcasted_iota(jnp.int32, (BLOCK, channels), 1) // HEAD_CHANNELS

    def per_head(block):
        if heads == 1:
            return block
        return jnp.concatenate(
            [jnp.where(lane == h, block, jnp.zeros_like(block)) for h in range(heads)], axis=0
        )

    rows = lax.broadcasted_iota(jnp.int32, (BLOCK, heads * BLOCK), 0)
    cols = lax.broadcasted_iota(jnp.int32, (BLOCK, heads * BLOCK), 1) % BLOCK
    lower = rows >= cols
    sum_rows = lax.broadcasted_iota(jnp.int32, (BLOCK, 3 * BLOCK), 0)
    sum_cols = lax.broadcasted_iota(jnp.int32, (BLOCK, 3 * BLOCK), 1) % BLOCK
    summing = (sum_rows >= sum_cols).astype(F32).astype(BF16)
    own_head = (
        lax.broadcasted_iota(jnp.int32, (channels, channels), 0) // HEAD_CHANNELS
        == lax.broadcasted_iota(jnp.int32, (channels, channels), 1) // HEAD_CHANNELS
    )
    margin = margin_ref[...]
    sudden = sudden_ref[...]
    sudden = jnp.concatenate([sudden, jnp.zeros((8 - heads, span), F32)], axis=0).T
    state = state_ref[...]
    total = total_ref[...]
    for j in range(span // BLOCK):
        at = pl.ds(j * BLOCK, BLOCK)
        strength = margin * jax.nn.sigmoid(-f_ref[at, :].astype(F32))
        extra = sudden[j * BLOCK : (j + 1) * BLOCK]
        jump = jnp.broadcast_to(extra[:, 0:1], (BLOCK, channels))
        for h in range(1, heads):
            jump = jnp.where(lane == h, jnp.broadcast_to(extra[:, h : h + 1], (BLOCK, channels)), jump)
        keep = jnp.log1p(-strength) + jump
        top = keep.astype(BF16)
        rest = keep - top.astype(F32)
        second = rest.astype(BF16)
        third = (rest - second.astype(F32)).astype(BF16)
        running = mm(summing, jnp.concatenate([top, second, third], axis=0))
        middle = running[BLOCK // 2 - 1 : BLOCK // 2]
        closing = running[BLOCK - 1 : BLOCK]
        scaled_q = q_ref[at, :].astype(F32) * jnp.exp(running - middle)
        scaled_k = strength * jnp.exp(middle - running)
        values = v_ref[at, :]
        scores = mm(scaled_q.astype(BF16), per_head(scaled_k.astype(BF16)), LANES_LANES)
        scores = jnp.where(lower, scores, 0.0).astype(BF16)
        lifted = scaled_q * jnp.exp(middle)
        local_ref[at, :] = mm(scores, per_head(values)) + mm(
            lifted.astype(BF16), state.astype(BF16), LANES_LANES
        )
        lifted_ref[at, :] = (lifted * jnp.exp(total)).astype(BF16)
        closed_k = (scaled_k * jnp.exp(closing - middle)).astype(BF16)
        added = mm(values, closed_k, ROWS_ROWS)
        state = state * jnp.exp(closing) + jnp.where(own_head, added, 0.0)
        total = total + closing
    state_ref[...] = state
    total_ref[...] = total
    final_ref[0:channels, :] = state
    final_ref[channels:, :] = jnp.broadcast_to(jnp.exp(total), (8, channels))


def scan_call(q, f, v, margin, sudden):
    tokens, channels = q.shape
    heads = channels // HEAD_CHANNELS
    span = min(tokens, 512)
    block = pl.BlockSpec((span, channels), lambda i: (i, 0))
    return pl.pallas_call(
        scan_kernel,
        grid=(tokens // span,),
        in_specs=[
            block,
            block,
            block,
            pl.BlockSpec((1, channels), lambda i: (0, 0)),
            pl.BlockSpec((heads, span), lambda i: (0, i)),
        ],
        out_specs=[block, block, pl.BlockSpec((channels + 8, channels), lambda i: (0, 0))],
        out_shape=[
            jax.ShapeDtypeStruct((tokens, channels), F32),
            jax.ShapeDtypeStruct((tokens, channels), BF16),
            jax.ShapeDtypeStruct((channels + 8, channels), F32),
        ],
        scratch_shapes=[pltpu.VMEM((channels, channels), F32), pltpu.VMEM((1, channels), F32)],
        compiler_params=pltpu.CompilerParams(dimension_semantics=("arbitrary",)),
        cost_estimate=pl.CostEstimate(
            flops=tokens * channels * 2000, bytes_accessed=tokens * channels * 14, transcendentals=0
        ),
        name="scan",
    )(q, f, v, margin.reshape(1, channels), sudden)


def gate_kernel(mine_ref, local_ref, lifted_ref, open_ref, pieces_ref, gain_ref, mixed_ref):
    span, channels = local_ref.shape
    mine = mine_ref[0]
    incoming = jnp.zeros((channels, channels), F32)
    for j in range(pieces_ref.shape[0] - 1):
        longer = incoming * pieces_ref[j, channels : channels + 1, :] + pieces_ref[j, 0:channels, :]
        incoming = jnp.where(j < mine, longer, incoming)
    heads_out = local_ref[...] + mm(lifted_ref[...], incoming.astype(BF16), LANES_LANES)
    own_head = (
        lax.broadcasted_iota(jnp.int32, (channels, channels), 0) // HEAD_CHANNELS
        == lax.broadcasted_iota(jnp.int32, (channels, channels), 1) // HEAD_CHANNELS
    )
    averaging = jnp.where(own_head, 1.0 / HEAD_CHANNELS, 0.0).astype(BF16)
    square = heads_out * heads_out
    top = square.astype(BF16)
    rest = (square - top.astype(F32)).astype(BF16)
    mean = mm(top, averaging) + mm(rest, averaging)
    opening = jax.nn.sigmoid(open_ref[...].astype(F32))
    mixed_ref[...] = (heads_out * lax.rsqrt(mean + EPS) * gain_ref[...] * opening).astype(BF16)


def gate_call(mine, local, lifted, opening, pieces, gain):
    tokens, channels = local.shape
    span = min(tokens, 1024)
    block = pl.BlockSpec((span, channels), lambda i: (i, 0))
    return pl.pallas_call(
        gate_kernel,
        grid=(tokens // span,),
        in_specs=[
            pl.BlockSpec(memory_space=pltpu.SMEM),
            block,
            block,
            block,
            pl.BlockSpec(pieces.shape, lambda i: (0, 0, 0)),
            pl.BlockSpec((1, channels), lambda i: (0, 0)),
        ],
        out_specs=block,
        out_shape=jax.ShapeDtypeStruct((tokens, channels), BF16),
        compiler_params=pltpu.CompilerParams(dimension_semantics=("arbitrary",)),
        cost_estimate=pl.CostEstimate(
            flops=tokens * channels * 800, bytes_accessed=tokens * channels * 10, transcendentals=0
        ),
        name="gate",
    )(mine, local, lifted, opening, pieces, gain)


def project_kernel(mixed_ref, weight_ref, residual_ref, mixer_ref, gain_ref, stream_ref, normed_ref):
    mixed = jnp.concatenate([mixed_ref[j] for j in range(mixed_ref.shape[0])], axis=1)
    projected = mm(mixed, weight_ref[...]).astype(BF16).astype(F32)
    stream = (residual_ref[...].astype(F32) + rms_scale(projected) * mixer_ref[...]).astype(BF16)
    stream_ref[...] = stream
    normed_ref[...] = (rms_scale(stream.astype(F32)) * gain_ref[...]).astype(BF16)


def project_call(mixed, weight, residual, mixer_gain, gain):
    sources, rows, channels = mixed.shape
    width = weight.shape[1]
    span = min(rows, 256)
    block = pl.BlockSpec((span, width), lambda i: (i, 0))
    vector = pl.BlockSpec((1, width), lambda i: (0, 0))
    return pl.pallas_call(
        project_kernel,
        grid=(rows // span,),
        in_specs=[
            pl.BlockSpec((sources, span, channels), lambda i: (0, i, 0)),
            pl.BlockSpec(weight.shape, lambda i: (0, 0)),
            block,
            vector,
            vector,
        ],
        out_specs=[block, block],
        out_shape=[jax.ShapeDtypeStruct((rows, width), BF16)] * 2,
        compiler_params=pltpu.CompilerParams(dimension_semantics=("arbitrary",)),
        cost_estimate=pl.CostEstimate(
            flops=2 * rows * width * weight.shape[0],
            bytes_accessed=2 * weight.size + 8 * rows * width,
            transcendentals=0,
        ),
        name="project",
    )(mixed, weight, residual, mixer_gain.reshape(1, width), gain.reshape(1, width))


def expert_kernel(rows_ref, share_ref, weights_ref, out_ref, sum_ref):
    expert, piece = pl.program_id(0), pl.program_id(1)
    first = jnp.logical_and(expert == 0, piece == 0)
    last = jnp.logical_and(expert == pl.num_programs(0) - 1, piece == pl.num_programs(1) - 1)
    rows = rows_ref[...]

    def joined(which):
        return jnp.concatenate([weights_ref[0, j, which] for j in range(weights_ref.shape[1])], axis=1)

    share = share_ref[...]
    lanes = lax.broadcasted_iota(jnp.int32, share.shape, 1)
    share = jnp.sum(jnp.where(lanes == expert, share, 0.0), axis=1, keepdims=True)
    gate = mm(rows, joined(0))
    up = mm(rows, joined(1))
    hidden = (gate * jax.nn.sigmoid(gate) * up * share).astype(BF16)
    added = mm(hidden, joined(2), LANES_LANES)

    @pl.when(first)
    def _():
        sum_ref[...] = added

    @pl.when(jnp.logical_not(first))
    def _():
        sum_ref[...] += added

    @pl.when(last)
    def _():
        out_ref[...] = sum_ref[...].astype(out_ref.dtype)


def expert_call(rows, share, weights, kind, name):
    count, width = rows.shape
    experts, shards, parts, _, units = weights.shape
    together = 2
    return pl.pallas_call(
        expert_kernel,
        grid=(experts, shards // together),
        in_specs=[
            pl.BlockSpec((count, width), lambda e, s: (0, 0)),
            pl.BlockSpec(share.shape, lambda e, s: (0, 0)),
            pl.BlockSpec((1, together, parts, width, units), lambda e, s: (e, s, 0, 0, 0)),
        ],
        out_specs=pl.BlockSpec((count, width), lambda e, s: (0, 0)),
        out_shape=jax.ShapeDtypeStruct((count, width), kind),
        scratch_shapes=[pltpu.VMEM((count, width), F32)],
        compiler_params=pltpu.CompilerParams(
            dimension_semantics=("arbitrary", "arbitrary"), vmem_limit_bytes=48 * 1024 * 1024
        ),
        cost_estimate=pl.CostEstimate(
            flops=2 * count * weights.size, bytes_accessed=2 * weights.size, transcendentals=0
        ),
        name=name,
    )(rows, share, weights)


def shared_expert(normed, gate_w, up_w, down_w):
    hidden = (
        jax.nn.silu(jnp.dot(normed, gate_w, preferred_element_type=F32))
        * jnp.dot(normed, up_w, preferred_element_type=F32)
    ).astype(BF16)
    return jnp.dot(hidden, down_w, preferred_element_type=F32)


def expert_rows(slot_rows, gate_w, up_w, down_w):
    hidden = (
        jax.nn.silu(jnp.dot(slot_rows, gate_w, preferred_element_type=F32))
        * jnp.dot(slot_rows, up_w, preferred_element_type=F32)
    ).astype(BF16)
    return lax.dot_general(hidden, down_w, LANES_LANES, preferred_element_type=F32)


def routed_by_slots(normed, index, weight, gate_w, up_w, down_w, sp):
    rows_here, routes_each = index.shape
    experts_all = lax.axis_size(sp)
    capacity = 3 * rows_here * routes_each // (2 * experts_all)
    numbers = jnp.arange(experts_all, dtype=jnp.int32)
    matches = (index[:, :, None] == numbers).astype(F32)
    hits = jnp.sum(matches, axis=1)
    strictly_lower = jnp.tril(jnp.ones((rows_here, rows_here), F32), -1)
    before_hits = jnp.dot(strictly_lower, hits, precision=TOP_PRECISION)
    slots = jnp.sum(before_hits[:, None, :] * matches, axis=2).astype(jnp.int32)
    targets = index * capacity + slots
    slot_numbers = jnp.arange(experts_all * capacity, dtype=jnp.int32)
    selector = (targets[:, :, None] == slot_numbers).astype(BF16)
    outgoing = jnp.einsum("rks,rd->sd", selector, normed, preferred_element_type=F32)
    outgoing = outgoing.astype(BF16).reshape(experts_all, capacity, normed.shape[1])
    arrived = lax.all_to_all(outgoing, sp, split_axis=0, concat_axis=0, tiled=True)
    sources, items, width = arrived.shape
    slot_rows = arrived.reshape(sources * items, width)
    gate_piece = lax.all_gather(gate_w, "tp", axis=2, tiled=True)[0]
    up_piece = lax.all_gather(up_w, "tp", axis=2, tiled=True)[0]
    down_piece = lax.all_gather(down_w, "tp", axis=2, tiled=True)[0]
    produced = expert_rows(slot_rows, gate_piece, up_piece, down_piece)
    results = produced.astype(BF16).reshape(sources, items, width)
    answered = lax.all_to_all(results, sp, split_axis=0, concat_axis=0, tiled=True)
    flat_answers = answered.reshape(experts_all * capacity, normed.shape[1])
    per_route = jnp.einsum("rks,sd->rkd", selector, flat_answers, preferred_element_type=F32)
    return jnp.sum(per_route * weight[:, :, None], axis=1)


def body(
    residual,
    query_values,
    forget_preact,
    value_written,
    output_gate_preact,
    forget_margin,
    sudden_decay,
    head_norm_gain,
    output_weight_matrix,
    mixer_norm_gain,
    feedforward_gain,
    routed_expert_index,
    routed_expert_weight,
    expert_gate_matrix,
    expert_up_matrix,
    expert_down_matrix,
    common_gate_matrix,
    common_up_matrix,
    common_down_matrix,
    final_norm_gain,
    *,
    sp,
):
    tokens, channels = query_values.shape
    rows = residual.shape[0]
    peers = lax.axis_size("tp")
    paired = len(sp) == 2
    if paired:
        outer, inner = sp
        packed = jnp.concatenate([expert_gate_matrix, expert_up_matrix, expert_down_matrix], axis=0)
        held = lax.all_gather(packed, (inner, "tp"))
        held = held.reshape((lax.axis_size(inner), peers) + packed.shape)
        experts_all = lax.axis_size(outer) * lax.axis_size(inner)
        numbers = jnp.arange(experts_all, dtype=jnp.int32)
        share = jnp.sum(
            (routed_expert_index[:, :, None] == numbers) * routed_expert_weight[:, :, None], axis=1
        )
        share = share.reshape(rows, lax.axis_size(outer), lax.axis_size(inner))
        swap = [(0, 1), (1, 0)]
        here = lax.axis_index(outer)
        own_share = jnp.where(here == 0, share[:, 0], share[:, 1])
        far_share = lax.ppermute(jnp.where(here == 0, share[:, 1], share[:, 0]), outer, swap)

    local, lifted, final = scan_call(
        query_values, forget_preact, value_written, forget_margin, sudden_decay
    )
    pieces = lax.all_gather(final, sp)
    mine = lax.axis_index(sp).reshape(1)
    gain = jnp.tile(head_norm_gain, channels // HEAD_CHANNELS).reshape(1, channels)
    mixed = gate_call(mine, local, lifted, output_gate_preact, pieces, gain)
    mixed = lax.all_to_all(
        mixed.reshape(peers, tokens // peers, channels), "tp", split_axis=0, concat_axis=0, tiled=True
    )
    if channels % 128 == 0:
        stream, normed = project_call(
            mixed, output_weight_matrix, residual, mixer_norm_gain, feedforward_gain
        )
    else:
        mixed = mixed.transpose(1, 0, 2).reshape(rows, peers * channels)
        projected = jnp.dot(mixed, output_weight_matrix, preferred_element_type=F32).astype(BF16)
        stream = (residual.astype(F32) + rms_scale(projected.astype(F32)) * mixer_norm_gain).astype(BF16)
        normed = (rms_scale(stream.astype(F32)) * feedforward_gain).astype(BF16)
    shared = shared_expert(normed, common_gate_matrix, common_up_matrix, common_down_matrix)
    if not paired:
        routed = routed_by_slots(
            normed,
            routed_expert_index,
            routed_expert_weight,
            expert_gate_matrix,
            expert_up_matrix,
            expert_down_matrix,
            sp,
        )
        layer_out = stream.astype(F32) + rms_scale(shared + routed) * final_norm_gain
        return layer_out.astype(BF16)
    far_rows = lax.ppermute(normed, outer, swap)
    chunks = 2
    part = rows // chunks
    answers = []
    for c in range(chunks):
        cut = slice(c * part, (c + 1) * part)
        partial = expert_call(far_rows[cut], far_share[cut], held, BF16, "far%d" % c)
        answers.append(lax.ppermute(partial, outer, swap))
    own = expert_call(normed, own_share, held, F32, "own")
    base = shared + own
    outs = []
    for c in range(chunks):
        cut = slice(c * part, (c + 1) * part)
        summed = base[cut] + answers[c].astype(F32)
        outs.append((stream[cut].astype(F32) + rms_scale(summed) * final_norm_gain).astype(BF16))
    return jnp.concatenate(outs, axis=0)


def solution(mesh):
    sp_size, tp_size = mesh.shape["sp"], mesh.shape["tp"]
    if sp_size == 4:
        sp = ("far", "near")
        mesh = Mesh(mesh.devices.reshape(2, 2, tp_size), sp + ("tp",))
    else:
        sp = ("sp",)
    every = P(sp + ("tp",), None)
    split = P(sp, "tp")
    shard = P(sp, None, "tp")
    placed = (
        every,
        split,
        split,
        split,
        split,
        P("tp"),
        P("tp", sp),
        P(),
        P(),
        P(),
        P(),
        every,
        every,
        shard,
        shard,
        shard,
        P(),
        P(),
        P(),
        P(),
    )
    return jax.shard_map(
        functools.partial(body, sp=sp), mesh=mesh, in_specs=placed, out_specs=every, check_vma=False
    )
```

```python
import functools

import jax
import jax.numpy as jnp
from jax import lax
from jax.experimental import pallas as pl
from jax.experimental.pallas import tpu as pltpu
from jax.sharding import Mesh, PartitionSpec as P

HEAD_CHANNELS = 64
BLOCK = 64
EPS = 1e-06
TOP_PRECISION = lax.Precision.HIGHEST
F32 = jnp.float32
BF16 = jnp.bfloat16

LANES_LANES = (((1,), (1,)), ((), ()))
ROWS_ROWS = (((0,), (0,)), ((), ()))


def rms_scale(values):
    return values * lax.rsqrt(jnp.mean(values * values, axis=-1, keepdims=True) + EPS)


def mm(a, b, dims=(((1,), (0,)), ((), ()))):
    return lax.dot_general(a, b, dims, preferred_element_type=F32)


def halves(value):
    top = value.astype(BF16)
    return top, (value - top.astype(F32)).astype(BF16)


def fine_mm(a, b):
    a_top, a_rest = a
    b_top, b_rest = b
    return mm(
        jnp.concatenate([a_top, a_rest, a_top], axis=1),
        jnp.concatenate([b_top, b_top, b_rest], axis=1),
        LANES_LANES,
    )


def scan_kernel(
    q_ref, f_ref, v_ref, margin_ref, sudden_ref, local_ref, lifted_ref, final_ref, state_ref, total_ref
):
    step = pl.program_id(0)
    span, channels = q_ref.shape
    heads = channels // HEAD_CHANNELS

    @pl.when(step == 0)
    def _():
        state_ref[...] = jnp.zeros_like(state_ref)
        total_ref[...] = jnp.zeros_like(total_ref)

    lane = lax.broadcasted_iota(jnp.int32, (BLOCK, channels), 1) // HEAD_CHANNELS

    def per_head(block):
        if heads == 1:
            return block
        return jnp.concatenate(
            [jnp.where(lane == h, block, jnp.zeros_like(block)) for h in range(heads)], axis=0
        )

    rows = lax.broadcasted_iota(jnp.int32, (BLOCK, heads * BLOCK), 0)
    cols = lax.broadcasted_iota(jnp.int32, (BLOCK, heads * BLOCK), 1) % BLOCK
    lower = rows >= cols
    sum_rows = lax.broadcasted_iota(jnp.int32, (BLOCK, 3 * BLOCK), 0)
    sum_cols = lax.broadcasted_iota(jnp.int32, (BLOCK, 3 * BLOCK), 1) % BLOCK
    summing = (sum_rows >= sum_cols).astype(F32).astype(BF16)
    own_head = (
        lax.broadcasted_iota(jnp.int32, (channels, channels), 0) // HEAD_CHANNELS
        == lax.broadcasted_iota(jnp.int32, (channels, channels), 1) // HEAD_CHANNELS
    )
    margin = margin_ref[...]
    sudden = sudden_ref[...]
    sudden = jnp.concatenate([sudden, jnp.zeros((8 - heads, span), F32)], axis=0).T
    state = state_ref[...]
    total = total_ref[...]
    for j in range(span // BLOCK):
        at = pl.ds(j * BLOCK, BLOCK)
        strength = margin * jax.nn.sigmoid(-f_ref[at, :].astype(F32))
        extra = sudden[j * BLOCK : (j + 1) * BLOCK]
        jump = jnp.broadcast_to(extra[:, 0:1], (BLOCK, channels))
        for h in range(1, heads):
            jump = jnp.where(lane == h, jnp.broadcast_to(extra[:, h : h + 1], (BLOCK, channels)), jump)
        keep = jnp.log1p(-strength) + jump
        top = keep.astype(BF16)
        rest = keep - top.astype(F32)
        second = rest.astype(BF16)
        third = (rest - second.astype(F32)).astype(BF16)
        running = mm(summing, jnp.concatenate([top, second, third], axis=0))
        middle = running[BLOCK // 2 - 1 : BLOCK // 2]
        closing = running[BLOCK - 1 : BLOCK]
        scaled_q = q_ref[at, :].astype(F32) * jnp.exp(running - middle)
        scaled_k = strength * jnp.exp(middle - running)
        values = v_ref[at, :]
        k_top, k_rest = halves(scaled_k)
        scores = fine_mm(halves(scaled_q), (per_head(k_top), per_head(k_rest)))
        score_top, score_rest = halves(jnp.where(lower, scores, 0.0))
        spread = per_head(values)
        lifted = scaled_q * jnp.exp(middle)
        local_ref[at, :] = mm(
            jnp.concatenate([score_top, score_rest], axis=1), jnp.concatenate([spread, spread], axis=0)
        ) + fine_mm(halves(lifted), halves(state))
        lifted_ref[at, :] = lifted * jnp.exp(total)
        closed_k = jnp.concatenate(halves(scaled_k * jnp.exp(closing - middle)), axis=0)
        added = mm(jnp.concatenate([values, values], axis=0), closed_k, ROWS_ROWS)
        state = state * jnp.exp(closing) + jnp.where(own_head, added, 0.0)
        total = total + closing
    state_ref[...] = state
    total_ref[...] = total
    final_ref[0:channels, :] = state
    final_ref[channels:, :] = jnp.broadcast_to(jnp.exp(total), (8, channels))


def scan_call(q, f, v, margin, sudden):
    tokens, channels = q.shape
    heads = channels // HEAD_CHANNELS
    span = min(tokens, 512)
    block = pl.BlockSpec((span, channels), lambda i: (i, 0))
    return pl.pallas_call(
        scan_kernel,
        grid=(tokens // span,),
        in_specs=[
            block,
            block,
            block,
            pl.BlockSpec((1, channels), lambda i: (0, 0)),
            pl.BlockSpec((heads, span), lambda i: (0, i)),
        ],
        out_specs=[block, block, pl.BlockSpec((channels + 8, channels), lambda i: (0, 0))],
        out_shape=[
            jax.ShapeDtypeStruct((tokens, channels), F32),
            jax.ShapeDtypeStruct((tokens, channels), F32),
            jax.ShapeDtypeStruct((channels + 8, channels), F32),
        ],
        scratch_shapes=[pltpu.VMEM((channels, channels), F32), pltpu.VMEM((1, channels), F32)],
        compiler_params=pltpu.CompilerParams(dimension_semantics=("arbitrary",)),
        cost_estimate=pl.CostEstimate(
            flops=tokens * channels * 2000, bytes_accessed=tokens * channels * 14, transcendentals=0
        ),
        name="scan",
    )(q, f, v, margin.reshape(1, channels), sudden)


def gate_kernel(mine_ref, local_ref, lifted_ref, open_ref, pieces_ref, gain_ref, mixed_ref):
    span, channels = local_ref.shape
    mine = mine_ref[0]
    incoming = jnp.zeros((channels, channels), F32)
    for j in range(pieces_ref.shape[0] - 1):
        longer = incoming * pieces_ref[j, channels : channels + 1, :] + pieces_ref[j, 0:channels, :]
        incoming = jnp.where(j < mine, longer, incoming)
    heads_out = local_ref[...] + fine_mm(halves(lifted_ref[...]), halves(incoming))
    own_head = (
        lax.broadcasted_iota(jnp.int32, (channels, channels), 0) // HEAD_CHANNELS
        == lax.broadcasted_iota(jnp.int32, (channels, channels), 1) // HEAD_CHANNELS
    )
    averaging = jnp.where(own_head, 1.0 / HEAD_CHANNELS, 0.0).astype(BF16)
    square = heads_out * heads_out
    top = square.astype(BF16)
    rest = (square - top.astype(F32)).astype(BF16)
    mean = mm(top, averaging) + mm(rest, averaging)
    opening = jax.nn.sigmoid(open_ref[...].astype(F32))
    mixed_ref[...] = (heads_out * lax.rsqrt(mean + EPS) * gain_ref[...] * opening).astype(BF16)


def gate_call(mine, local, lifted, opening, pieces, gain):
    tokens, channels = local.shape
    span = min(tokens, 1024)
    block = pl.BlockSpec((span, channels), lambda i: (i, 0))
    return pl.pallas_call(
        gate_kernel,
        grid=(tokens // span,),
        in_specs=[
            pl.BlockSpec(memory_space=pltpu.SMEM),
            block,
            block,
            block,
            pl.BlockSpec(pieces.shape, lambda i: (0, 0, 0)),
            pl.BlockSpec((1, channels), lambda i: (0, 0)),
        ],
        out_specs=block,
        out_shape=jax.ShapeDtypeStruct((tokens, channels), BF16),
        compiler_params=pltpu.CompilerParams(dimension_semantics=("arbitrary",)),
        cost_estimate=pl.CostEstimate(
            flops=tokens * channels * 800, bytes_accessed=tokens * channels * 10, transcendentals=0
        ),
        name="gate",
    )(mine, local, lifted, opening, pieces, gain)


def project_kernel(mixed_ref, weight_ref, residual_ref, mixer_ref, gain_ref, stream_ref, normed_ref):
    mixed = jnp.concatenate([mixed_ref[j] for j in range(mixed_ref.shape[0])], axis=1)
    projected = mm(mixed, weight_ref[...]).astype(BF16).astype(F32)
    stream = (residual_ref[...].astype(F32) + rms_scale(projected) * mixer_ref[...]).astype(BF16)
    stream_ref[...] = stream
    normed_ref[...] = (rms_scale(stream.astype(F32)) * gain_ref[...]).astype(BF16)


def project_call(mixed, weight, residual, mixer_gain, gain):
    sources, rows, channels = mixed.shape
    width = weight.shape[1]
    span = min(rows, 256)
    block = pl.BlockSpec((span, width), lambda i: (i, 0))
    vector = pl.BlockSpec((1, width), lambda i: (0, 0))
    return pl.pallas_call(
        project_kernel,
        grid=(rows // span,),
        in_specs=[
            pl.BlockSpec((sources, span, channels), lambda i: (0, i, 0)),
            pl.BlockSpec(weight.shape, lambda i: (0, 0)),
            block,
            vector,
            vector,
        ],
        out_specs=[block, block],
        out_shape=[jax.ShapeDtypeStruct((rows, width), BF16)] * 2,
        compiler_params=pltpu.CompilerParams(dimension_semantics=("arbitrary",)),
        cost_estimate=pl.CostEstimate(
            flops=2 * rows * width * weight.shape[0],
            bytes_accessed=2 * weight.size + 8 * rows * width,
            transcendentals=0,
        ),
        name="project",
    )(mixed, weight, residual, mixer_gain.reshape(1, width), gain.reshape(1, width))


def pack_kernel(gate_ref, up_ref, down_ref, packed_ref):
    width, units = gate_ref.shape[1:]
    packed_ref[0:width, 0:units] = gate_ref[0]
    packed_ref[0:width, units:] = up_ref[0]
    for j in range(width // (2 * units)):
        turned = down_ref[0, j * 2 * units : (j + 1) * 2 * units, :].T
        packed_ref[width + j * units : width + (j + 1) * units, :] = turned


def pack_call(gate, up, down):
    _, width, units = gate.shape
    return pl.pallas_call(
        pack_kernel,
        out_shape=jax.ShapeDtypeStruct((width + width // 2, 2 * units), gate.dtype),
        cost_estimate=pl.CostEstimate(flops=0, bytes_accessed=12 * width * units, transcendentals=0),
        name="pack",
    )(gate, up, down)


def expert_kernel(rows_ref, share_ref, weights_ref, out_ref, sum_ref):
    expert, piece = pl.program_id(0), pl.program_id(1)
    first = jnp.logical_and(expert == 0, piece == 0)
    last = jnp.logical_and(expert == pl.num_programs(0) - 1, piece == pl.num_programs(1) - 1)
    count, width = rows_ref.shape
    shards, _, double = weights_ref.shape[1:]
    units = double // 2

    @pl.when(first)
    def _():
        sum_ref[...] = jnp.zeros_like(sum_ref)

    share = share_ref[...]
    lanes = lax.broadcasted_iota(jnp.int32, share.shape, 1)
    share = jnp.sum(jnp.where(lanes == expert, share, 0.0), axis=1, keepdims=True)
    hidden = []
    for j in range(shards):
        both = mm(rows_ref[...], weights_ref[0, j, 0:width, :])
        gate, up = both[:, :units], both[:, units:]
        hidden.append((gate * jax.nn.sigmoid(gate) * up * share).astype(BF16))
    hidden = jnp.concatenate(hidden, axis=1)
    for c in range(width // double):
        at = slice(width + c * units, width + (c + 1) * units)
        down = jnp.concatenate([weights_ref[0, j, at, :] for j in range(shards)], axis=0)
        sum_ref[:, c * double : (c + 1) * double] += mm(hidden, down)

    @pl.when(last)
    def _():
        out_ref[...] = sum_ref[...].astype(out_ref.dtype)


def expert_call(rows, share, weights, kind, name, chunk, chunks):
    count, width = rows.shape
    count = count // chunks
    experts, shards, depth, double = weights.shape
    together = 2
    return pl.pallas_call(
        expert_kernel,
        grid=(experts, shards // together),
        in_specs=[
            pl.BlockSpec((count, width), lambda e, s: (chunk, 0)),
            pl.BlockSpec((count, share.shape[1]), lambda e, s: (chunk, 0)),
            pl.BlockSpec((1, together, depth, double), lambda e, s: (e, s, 0, 0)),
        ],
        out_specs=pl.BlockSpec((count, width), lambda e, s: (0, 0)),
        out_shape=jax.ShapeDtypeStruct((count, width), kind),
        scratch_shapes=[pltpu.VMEM((count, width), F32)],
        compiler_params=pltpu.CompilerParams(
            dimension_semantics=("arbitrary", "arbitrary"), vmem_limit_bytes=48 * 1024 * 1024
        ),
        cost_estimate=pl.CostEstimate(
            flops=2 * count * weights.size, bytes_accessed=2 * weights.size, transcendentals=0
        ),
        name=name,
    )(rows, share, weights)


def combine_kernel(*refs):
    stream_ref, shared_ref, own_ref, answer_ref, gain_ref, out_ref = refs[-6:]
    summed = shared_ref[...] + own_ref[...] + answer_ref[...].astype(F32)
    out_ref[...] = (stream_ref[...].astype(F32) + rms_scale(summed) * gain_ref[...]).astype(BF16)


def combine_call(so_far, stream, shared, own, answer, gain, chunk, chunks):
    rows, width = stream.shape
    span = min(rows // chunks, 128)
    steps = rows // chunks // span
    block = pl.BlockSpec((span, width), lambda i: (chunk * steps + i, 0))
    specs = [block, block, block, pl.BlockSpec((span, width), lambda i: (i, 0))]
    specs.append(pl.BlockSpec((1, width), lambda i: (0, 0)))
    operands = [stream, shared, own, answer, gain.reshape(1, width)]
    aliases = {}
    if so_far is not None:
        specs.insert(0, pl.BlockSpec(memory_space=pl.ANY))
        operands.insert(0, so_far)
        aliases = {0: 0}
    return pl.pallas_call(
        combine_kernel,
        grid=(steps,),
        in_specs=specs,
        out_specs=block,
        out_shape=jax.ShapeDtypeStruct((rows, width), BF16),
        input_output_aliases=aliases,
        compiler_params=pltpu.CompilerParams(dimension_semantics=("arbitrary",)),
        cost_estimate=pl.CostEstimate(
            flops=rows * width, bytes_accessed=14 * rows * width // chunks, transcendentals=0
        ),
        name="combine%d" % chunk,
    )(*operands)


def shared_expert(normed, gate_w, up_w, down_w):
    hidden = (
        jax.nn.silu(jnp.dot(normed, gate_w, preferred_element_type=F32))
        * jnp.dot(normed, up_w, preferred_element_type=F32)
    ).astype(BF16)
    return jnp.dot(hidden, down_w, preferred_element_type=F32)


def expert_rows(slot_rows, gate_w, up_w, down_w):
    hidden = (
        jax.nn.silu(jnp.dot(slot_rows, gate_w, preferred_element_type=F32))
        * jnp.dot(slot_rows, up_w, preferred_element_type=F32)
    ).astype(BF16)
    return lax.dot_general(hidden, down_w, LANES_LANES, preferred_element_type=F32)


def routed_by_slots(normed, index, weight, gate_w, up_w, down_w, sp):
    rows_here, routes_each = index.shape
    experts_all = lax.axis_size(sp)
    capacity = 3 * rows_here * routes_each // (2 * experts_all)
    numbers = jnp.arange(experts_all, dtype=jnp.int32)
    matches = (index[:, :, None] == numbers).astype(F32)
    hits = jnp.sum(matches, axis=1)
    strictly_lower = jnp.tril(jnp.ones((rows_here, rows_here), F32), -1)
    before_hits = jnp.dot(strictly_lower, hits, precision=TOP_PRECISION)
    slots = jnp.sum(before_hits[:, None, :] * matches, axis=2).astype(jnp.int32)
    targets = index * capacity + slots
    slot_numbers = jnp.arange(experts_all * capacity, dtype=jnp.int32)
    selector = (targets[:, :, None] == slot_numbers).astype(BF16)
    outgoing = jnp.einsum("rks,rd->sd", selector, normed, preferred_element_type=F32)
    outgoing = outgoing.astype(BF16).reshape(experts_all, capacity, normed.shape[1])
    arrived = lax.all_to_all(outgoing, sp, split_axis=0, concat_axis=0, tiled=True)
    sources, items, width = arrived.shape
    slot_rows = arrived.reshape(sources * items, width)
    gate_piece = lax.all_gather(gate_w, "tp", axis=2, tiled=True)[0]
    up_piece = lax.all_gather(up_w, "tp", axis=2, tiled=True)[0]
    down_piece = lax.all_gather(down_w, "tp", axis=2, tiled=True)[0]
    produced = expert_rows(slot_rows, gate_piece, up_piece, down_piece)
    results = produced.astype(BF16).reshape(sources, items, width)
    answered = lax.all_to_all(results, sp, split_axis=0, concat_axis=0, tiled=True)
    flat_answers = answered.reshape(experts_all * capacity, normed.shape[1])
    per_route = jnp.einsum("rks,sd->rkd", selector, flat_answers, preferred_element_type=F32)
    return jnp.sum(per_route * weight[:, :, None], axis=1)


def body(
    residual,
    query_values,
    forget_preact,
    value_written,
    output_gate_preact,
    forget_margin,
    sudden_decay,
    head_norm_gain,
    output_weight_matrix,
    mixer_norm_gain,
    feedforward_gain,
    routed_expert_index,
    routed_expert_weight,
    expert_gate_matrix,
    expert_up_matrix,
    expert_down_matrix,
    common_gate_matrix,
    common_up_matrix,
    common_down_matrix,
    final_norm_gain,
    *,
    sp,
):
    tokens, channels = query_values.shape
    rows = residual.shape[0]
    peers = lax.axis_size("tp")
    paired = len(sp) == 2
    if paired:
        outer, inner = sp
        packed = pack_call(expert_gate_matrix, expert_up_matrix, expert_down_matrix)
        held = lax.all_gather(packed, (inner, "tp"))
        held = held.reshape((lax.axis_size(inner), peers) + packed.shape)
        experts_all = lax.axis_size(outer) * lax.axis_size(inner)
        numbers = jnp.arange(experts_all, dtype=jnp.int32)
        share = jnp.sum(
            (routed_expert_index[:, :, None] == numbers) * routed_expert_weight[:, :, None], axis=1
        )
        share = share.reshape(rows, lax.axis_size(outer), lax.axis_size(inner))
        swap = [(0, 1), (1, 0)]
        here = lax.axis_index(outer)
        own_share = jnp.where(here == 0, share[:, 0], share[:, 1])
        far_share = lax.ppermute(jnp.where(here == 0, share[:, 1], share[:, 0]), outer, swap)

    local, lifted, final = scan_call(
        query_values, forget_preact, value_written, forget_margin, sudden_decay
    )
    pieces = lax.all_gather(final, sp)
    mine = lax.axis_index(sp).reshape(1)
    gain = jnp.tile(head_norm_gain, channels // HEAD_CHANNELS).reshape(1, channels)
    mixed = gate_call(mine, local, lifted, output_gate_preact, pieces, gain)
    mixed = lax.all_to_all(
        mixed.reshape(peers, tokens // peers, channels), "tp", split_axis=0, concat_axis=0, tiled=True
    )
    if channels % 128 == 0:
        stream, normed = project_call(
            mixed, output_weight_matrix, residual, mixer_norm_gain, feedforward_gain
        )
    else:
        mixed = mixed.transpose(1, 0, 2).reshape(rows, peers * channels)
        projected = jnp.dot(mixed, output_weight_matrix, preferred_element_type=F32).astype(BF16)
        stream = (residual.astype(F32) + rms_scale(projected.astype(F32)) * mixer_norm_gain).astype(BF16)
        normed = (rms_scale(stream.astype(F32)) * feedforward_gain).astype(BF16)
    shared = shared_expert(normed, common_gate_matrix, common_up_matrix, common_down_matrix)
    if not paired:
        routed = routed_by_slots(
            normed,
            routed_expert_index,
            routed_expert_weight,
            expert_gate_matrix,
            expert_up_matrix,
            expert_down_matrix,
            sp,
        )
        layer_out = stream.astype(F32) + rms_scale(shared + routed) * final_norm_gain
        return layer_out.astype(BF16)
    far_rows = lax.ppermute(normed, outer, swap)
    far_rows, shared = lax.optimization_barrier((far_rows, shared))
    chunks = 2
    answers = []
    for c in range(chunks):
        partial = expert_call(far_rows, far_share, held, BF16, "far%d" % c, c, chunks)
        answers.append(lax.ppermute(partial, outer, swap))
    own = expert_call(normed, own_share, held, F32, "own", 0, 1)
    layer_out = None
    for c in range(chunks):
        layer_out = combine_call(
            layer_out, stream, shared, own, answers[c], final_norm_gain, c, chunks
        )
    return layer_out


def solution(mesh):
    sp_size, tp_size = mesh.shape["sp"], mesh.shape["tp"]
    if sp_size == 4:
        sp = ("far", "near")
        mesh = Mesh(mesh.devices.reshape(2, 2, tp_size), sp + ("tp",))
    else:
        sp = ("sp",)
    every = P(sp + ("tp",), None)
    split = P(sp, "tp")
    shard = P(sp, None, "tp")
    placed = (
        every,
        split,
        split,
        split,
        split,
        P("tp"),
        P("tp", sp),
        P(),
        P(),
        P(),
        P(),
        every,
        every,
        shard,
        shard,
        shard,
        P(),
        P(),
        P(),
        P(),
    )
    return jax.shard_map(
        functools.partial(body, sp=sp), mesh=mesh, in_specs=placed, out_specs=every, check_vma=False
    )
```

```python
import functools

import jax
import jax.numpy as jnp
from jax import lax
from jax.experimental import pallas as pl
from jax.experimental.pallas import tpu as pltpu
from jax.sharding import Mesh, PartitionSpec as P

HEAD_CHANNELS = 64
BLOCK = 64
EPS = 1e-06
TOP_PRECISION = lax.Precision.HIGHEST
F32 = jnp.float32
BF16 = jnp.bfloat16

LANES_LANES = (((1,), (1,)), ((), ()))
ROWS_ROWS = (((0,), (0,)), ((), ()))


def rms_scale(values):
    return values * lax.rsqrt(jnp.mean(values * values, axis=-1, keepdims=True) + EPS)


def mm(a, b, dims=(((1,), (0,)), ((), ()))):
    return lax.dot_general(a, b, dims, preferred_element_type=F32)


def halves(value):
    top = value.astype(BF16)
    return top, (value - top.astype(F32)).astype(BF16)


def fine_mm(a, b):
    a_top, a_rest = a
    b_top, b_rest = b
    return mm(
        jnp.concatenate([a_top, a_rest, a_top], axis=1),
        jnp.concatenate([b_top, b_top, b_rest], axis=1),
        LANES_LANES,
    )


def scan_kernel(
    q_ref, f_ref, v_ref, margin_ref, sudden_ref, local_ref, lifted_ref, final_ref, state_ref, total_ref
):
    step = pl.program_id(0)
    span, channels = q_ref.shape
    heads = channels // HEAD_CHANNELS

    @pl.when(step == 0)
    def _():
        state_ref[...] = jnp.zeros_like(state_ref)
        total_ref[...] = jnp.zeros_like(total_ref)

    lane = lax.broadcasted_iota(jnp.int32, (BLOCK, channels), 1) // HEAD_CHANNELS

    def per_head(block):
        if heads == 1:
            return block
        return jnp.concatenate(
            [jnp.where(lane == h, block, jnp.zeros_like(block)) for h in range(heads)], axis=0
        )

    rows = lax.broadcasted_iota(jnp.int32, (BLOCK, heads * BLOCK), 0)
    cols = lax.broadcasted_iota(jnp.int32, (BLOCK, heads * BLOCK), 1) % BLOCK
    lower = rows >= cols
    sum_rows = lax.broadcasted_iota(jnp.int32, (BLOCK, 3 * BLOCK), 0)
    sum_cols = lax.broadcasted_iota(jnp.int32, (BLOCK, 3 * BLOCK), 1) % BLOCK
    summing = (sum_rows >= sum_cols).astype(F32).astype(BF16)
    own_head = (
        lax.broadcasted_iota(jnp.int32, (channels, channels), 0) // HEAD_CHANNELS
        == lax.broadcasted_iota(jnp.int32, (channels, channels), 1) // HEAD_CHANNELS
    )
    margin = margin_ref[...]
    sudden = sudden_ref[...]
    sudden = jnp.concatenate([sudden, jnp.zeros((8 - heads, span), F32)], axis=0).T
    state = state_ref[...]
    total = total_ref[...]
    for j in range(span // BLOCK):
        at = pl.ds(j * BLOCK, BLOCK)
        strength = margin * jax.nn.sigmoid(-f_ref[at, :].astype(F32))
        extra = sudden[j * BLOCK : (j + 1) * BLOCK]
        jump = jnp.broadcast_to(extra[:, 0:1], (BLOCK, channels))
        for h in range(1, heads):
            jump = jnp.where(lane == h, jnp.broadcast_to(extra[:, h : h + 1], (BLOCK, channels)), jump)
        keep = jnp.log1p(-strength) + jump
        top = keep.astype(BF16)
        rest = keep - top.astype(F32)
        second = rest.astype(BF16)
        third = (rest - second.astype(F32)).astype(BF16)
        running = mm(summing, jnp.concatenate([top, second, third], axis=0))
        middle = running[BLOCK // 2 - 1 : BLOCK // 2]
        closing = running[BLOCK - 1 : BLOCK]
        scaled_q = q_ref[at, :].astype(F32) * jnp.exp(running - middle)
        scaled_k = strength * jnp.exp(middle - running)
        values = v_ref[at, :]
        k_top, k_rest = halves(scaled_k)
        scores = fine_mm(halves(scaled_q), (per_head(k_top), per_head(k_rest)))
        score_top, score_rest = halves(jnp.where(lower, scores, 0.0))
        spread = per_head(values)
        lifted = scaled_q * jnp.exp(middle)
        local_ref[at, :] = mm(
            jnp.concatenate([score_top, score_rest], axis=1), jnp.concatenate([spread, spread], axis=0)
        ) + fine_mm(halves(lifted), halves(state))
        lifted_ref[at, :] = lifted * jnp.exp(total)
        closed_k = jnp.concatenate(halves(scaled_k * jnp.exp(closing - middle)), axis=0)
        added = mm(jnp.concatenate([values, values], axis=0), closed_k, ROWS_ROWS)
        state = state * jnp.exp(closing) + jnp.where(own_head, added, 0.0)
        total = total + closing
    state_ref[...] = state
    total_ref[...] = total
    final_ref[0:channels, :] = state
    final_ref[channels:, :] = jnp.broadcast_to(jnp.exp(total), (8, channels))


def scan_call(q, f, v, margin, sudden):
    tokens, channels = q.shape
    heads = channels // HEAD_CHANNELS
    span = min(tokens, 512)
    block = pl.BlockSpec((span, channels), lambda i: (i, 0))
    return pl.pallas_call(
        scan_kernel,
        grid=(tokens // span,),
        in_specs=[
            block,
            block,
            block,
            pl.BlockSpec((1, channels), lambda i: (0, 0)),
            pl.BlockSpec((heads, span), lambda i: (0, i)),
        ],
        out_specs=[block, block, pl.BlockSpec((channels + 8, channels), lambda i: (0, 0))],
        out_shape=[
            jax.ShapeDtypeStruct((tokens, channels), F32),
            jax.ShapeDtypeStruct((tokens, channels), F32),
            jax.ShapeDtypeStruct((channels + 8, channels), F32),
        ],
        scratch_shapes=[pltpu.VMEM((channels, channels), F32), pltpu.VMEM((1, channels), F32)],
        compiler_params=pltpu.CompilerParams(dimension_semantics=("arbitrary",)),
        cost_estimate=pl.CostEstimate(
            flops=tokens * channels * 2000, bytes_accessed=tokens * channels * 14, transcendentals=0
        ),
        name="scan",
    )(q, f, v, margin.reshape(1, channels), sudden)


def gate_kernel(mine_ref, local_ref, lifted_ref, open_ref, pieces_ref, gain_ref, mixed_ref):
    span, channels = local_ref.shape
    mine = mine_ref[0]
    incoming = jnp.zeros((channels, channels), F32)
    for j in range(pieces_ref.shape[0] - 1):
        longer = incoming * pieces_ref[j, channels : channels + 1, :] + pieces_ref[j, 0:channels, :]
        incoming = jnp.where(j < mine, longer, incoming)
    heads_out = local_ref[...] + fine_mm(halves(lifted_ref[...]), halves(incoming))
    own_head = (
        lax.broadcasted_iota(jnp.int32, (channels, channels), 0) // HEAD_CHANNELS
        == lax.broadcasted_iota(jnp.int32, (channels, channels), 1) // HEAD_CHANNELS
    )
    averaging = jnp.where(own_head, 1.0 / HEAD_CHANNELS, 0.0).astype(BF16)
    square = heads_out * heads_out
    top = square.astype(BF16)
    rest = (square - top.astype(F32)).astype(BF16)
    mean = mm(top, averaging) + mm(rest, averaging)
    opening = jax.nn.sigmoid(open_ref[...].astype(F32))
    mixed_ref[...] = (heads_out * lax.rsqrt(mean + EPS) * gain_ref[...] * opening).astype(BF16)


def gate_call(mine, local, lifted, opening, pieces, gain):
    tokens, channels = local.shape
    span = min(tokens, 1024)
    block = pl.BlockSpec((span, channels), lambda i: (i, 0))
    return pl.pallas_call(
        gate_kernel,
        grid=(tokens // span,),
        in_specs=[
            pl.BlockSpec(memory_space=pltpu.SMEM),
            block,
            block,
            block,
            pl.BlockSpec(pieces.shape, lambda i: (0, 0, 0)),
            pl.BlockSpec((1, channels), lambda i: (0, 0)),
        ],
        out_specs=block,
        out_shape=jax.ShapeDtypeStruct((tokens, channels), BF16),
        compiler_params=pltpu.CompilerParams(dimension_semantics=("arbitrary",)),
        cost_estimate=pl.CostEstimate(
            flops=tokens * channels * 800, bytes_accessed=tokens * channels * 10, transcendentals=0
        ),
        name="gate",
    )(mine, local, lifted, opening, pieces, gain)


def project_kernel(
    mixed_ref,
    weight_ref,
    residual_ref,
    mixer_ref,
    gain_ref,
    gate_ref,
    up_ref,
    down_ref,
    stream_ref,
    normed_ref,
    shared_ref,
):
    mixed = jnp.concatenate([mixed_ref[j] for j in range(mixed_ref.shape[0])], axis=1)
    projected = mm(mixed, weight_ref[...]).astype(BF16).astype(F32)
    stream = (residual_ref[...].astype(F32) + rms_scale(projected) * mixer_ref[...]).astype(BF16)
    stream_ref[...] = stream
    normed = (rms_scale(stream.astype(F32)) * gain_ref[...]).astype(BF16)
    normed_ref[...] = normed
    gate = mm(normed, gate_ref[...])
    hidden = (gate * jax.nn.sigmoid(gate) * mm(normed, up_ref[...])).astype(BF16)
    shared_ref[...] = mm(hidden, down_ref[...])


def project_call(mixed, weight, residual, mixer_gain, gain, shared_weights):
    sources, rows, channels = mixed.shape
    width = weight.shape[1]
    span = min(rows, 256)
    block = pl.BlockSpec((span, width), lambda i: (i, 0))

    def whole(array):
        return pl.BlockSpec(array.shape, lambda i: (0, 0))

    vectors = [mixer_gain.reshape(1, width), gain.reshape(1, width)]
    hidden = shared_weights[0].shape[1]
    return pl.pallas_call(
        project_kernel,
        grid=(rows // span,),
        in_specs=[pl.BlockSpec((sources, span, channels), lambda i: (0, i, 0)), whole(weight), block]
        + [whole(array) for array in vectors + list(shared_weights)],
        out_specs=[block, block, block],
        out_shape=[
            jax.ShapeDtypeStruct((rows, width), BF16),
            jax.ShapeDtypeStruct((rows, width), BF16),
            jax.ShapeDtypeStruct((rows, width), F32),
        ],
        compiler_params=pltpu.CompilerParams(
            dimension_semantics=("arbitrary",), vmem_limit_bytes=48 * 1024 * 1024
        ),
        cost_estimate=pl.CostEstimate(
            flops=2 * rows * width * (weight.shape[0] + 3 * hidden),
            bytes_accessed=2 * weight.size + 12 * rows * width,
            transcendentals=0,
        ),
        name="project",
    )(mixed, weight, residual, *vectors, *shared_weights)


def pack_kernel(gate_ref, up_ref, down_ref, packed_ref):
    width, units = gate_ref.shape[1:]
    packed_ref[0:width, 0:units] = gate_ref[0]
    packed_ref[0:width, units:] = up_ref[0]
    for j in range(width // (2 * units)):
        turned = down_ref[0, j * 2 * units : (j + 1) * 2 * units, :].T
        packed_ref[width + j * units : width + (j + 1) * units, :] = turned


def pack_call(gate, up, down):
    _, width, units = gate.shape
    return pl.pallas_call(
        pack_kernel,
        out_shape=jax.ShapeDtypeStruct((width + width // 2, 2 * units), gate.dtype),
        cost_estimate=pl.CostEstimate(flops=0, bytes_accessed=12 * width * units, transcendentals=0),
        name="pack",
    )(gate, up, down)


def expert_kernel(*refs, based):
    rows_ref, share_ref, weights_ref = refs[:3]
    out_refs, sum_ref = refs[3 + based : -1], refs[-1]
    expert, piece = pl.program_id(0), pl.program_id(1)
    first = jnp.logical_and(expert == 0, piece == 0)
    last = jnp.logical_and(expert == pl.num_programs(0) - 1, piece == pl.num_programs(1) - 1)
    width = rows_ref.shape[1]
    shards, _, double = weights_ref.shape[1:]
    units = double // 2

    @pl.when(first)
    def _():
        sum_ref[...] = jnp.zeros_like(sum_ref)

    share = share_ref[...].T
    lanes = lax.broadcasted_iota(jnp.int32, share.shape, 1)
    share = jnp.sum(jnp.where(lanes == expert, share, 0.0), axis=1, keepdims=True)
    hidden = []
    for j in range(shards):
        both = mm(rows_ref[...], weights_ref[0, j, 0:width, :])
        gate, up = both[:, :units], both[:, units:]
        hidden.append((gate * jax.nn.sigmoid(gate) * up * share).astype(BF16))
    hidden = jnp.concatenate(hidden, axis=1)
    for c in range(width // double):
        at = slice(width + c * units, width + (c + 1) * units)
        down = jnp.concatenate([weights_ref[0, j, at, :] for j in range(shards)], axis=0)
        sum_ref[:, c * double : (c + 1) * double] += mm(hidden, down)

    @pl.when(last)
    def _():
        start = 0
        for out_ref in out_refs:
            at = slice(start, start + out_ref.shape[0])
            total = sum_ref[at, :] + refs[3][at, :] if based else sum_ref[at, :]
            out_ref[...] = total.astype(out_ref.dtype)
            start += out_ref.shape[0]


def expert_call(rows, share, weights, base, pieces, kind, name, together):
    count, width = rows.shape
    experts, shards, depth, double = weights.shape

    def whole(size):
        return pl.BlockSpec((size, width), lambda e, s: (0, 0))

    specs = [
        whole(count),
        pl.BlockSpec(share.shape, lambda e, s: (0, 0)),
        pl.BlockSpec((1, together, depth, double), lambda e, s: (e, s, 0, 0)),
    ]
    operands = [rows, share, weights]
    if base is not None:
        specs.append(whole(count))
        operands.append(base)
    return pl.pallas_call(
        functools.partial(expert_kernel, based=base is not None),
        grid=(experts, shards // together),
        in_specs=specs,
        out_specs=[whole(size) for size in pieces],
        out_shape=[jax.ShapeDtypeStruct((size, width), kind) for size in pieces],
        scratch_shapes=[pltpu.VMEM((count, width), F32)],
        compiler_params=pltpu.CompilerParams(
            dimension_semantics=("arbitrary", "arbitrary"), vmem_limit_bytes=48 * 1024 * 1024
        ),
        cost_estimate=pl.CostEstimate(
            flops=2 * count * weights.size, bytes_accessed=2 * weights.size, transcendentals=0
        ),
        name=name,
    )(*operands)


def combine_kernel(*refs):
    stream_ref, base_ref, answer_ref, gain_ref, out_ref = refs[-5:]
    summed = base_ref[...] + answer_ref[...].astype(F32)
    out_ref[...] = (stream_ref[...].astype(F32) + rms_scale(summed) * gain_ref[...]).astype(BF16)


def combine_call(so_far, stream, base, answer, gain, start):
    rows, width = stream.shape
    span = min(answer.shape[0], 64)
    skip = start // span
    block = pl.BlockSpec((span, width), lambda i: (skip + i, 0))
    specs = [block, block, pl.BlockSpec((span, width), lambda i: (i, 0))]
    specs.append(pl.BlockSpec((1, width), lambda i: (0, 0)))
    operands = [stream, base, answer, gain.reshape(1, width)]
    aliases = {}
    if so_far is not None:
        specs.insert(0, pl.BlockSpec(memory_space=pl.ANY))
        operands.insert(0, so_far)
        aliases = {0: 0}
    return pl.pallas_call(
        combine_kernel,
        grid=(answer.shape[0] // span,),
        in_specs=specs,
        out_specs=block,
        out_shape=jax.ShapeDtypeStruct((rows, width), BF16),
        input_output_aliases=aliases,
        compiler_params=pltpu.CompilerParams(dimension_semantics=("arbitrary",)),
        cost_estimate=pl.CostEstimate(
            flops=answer.size, bytes_accessed=10 * answer.size, transcendentals=0
        ),
        name="combine%d" % start,
    )(*operands)


def shared_expert(normed, gate_w, up_w, down_w):
    hidden = (
        jax.nn.silu(jnp.dot(normed, gate_w, preferred_element_type=F32))
        * jnp.dot(normed, up_w, preferred_element_type=F32)
    ).astype(BF16)
    return jnp.dot(hidden, down_w, preferred_element_type=F32)


def expert_rows(slot_rows, gate_w, up_w, down_w):
    hidden = (
        jax.nn.silu(jnp.dot(slot_rows, gate_w, preferred_element_type=F32))
        * jnp.dot(slot_rows, up_w, preferred_element_type=F32)
    ).astype(BF16)
    return lax.dot_general(hidden, down_w, LANES_LANES, preferred_element_type=F32)


def routed_by_slots(normed, index, weight, gate_w, up_w, down_w, sp):
    rows_here, routes_each = index.shape
    experts_all = lax.axis_size(sp)
    capacity = 3 * rows_here * routes_each // (2 * experts_all)
    numbers = jnp.arange(experts_all, dtype=jnp.int32)
    matches = (index[:, :, None] == numbers).astype(F32)
    hits = jnp.sum(matches, axis=1)
    strictly_lower = jnp.tril(jnp.ones((rows_here, rows_here), F32), -1)
    before_hits = jnp.dot(strictly_lower, hits, precision=TOP_PRECISION)
    slots = jnp.sum(before_hits[:, None, :] * matches, axis=2).astype(jnp.int32)
    targets = index * capacity + slots
    slot_numbers = jnp.arange(experts_all * capacity, dtype=jnp.int32)
    selector = (targets[:, :, None] == slot_numbers).astype(BF16)
    outgoing = jnp.einsum("rks,rd->sd", selector, normed, preferred_element_type=F32)
    outgoing = outgoing.astype(BF16).reshape(experts_all, capacity, normed.shape[1])
    arrived = lax.all_to_all(outgoing, sp, split_axis=0, concat_axis=0, tiled=True)
    sources, items, width = arrived.shape
    slot_rows = arrived.reshape(sources * items, width)
    gate_piece = lax.all_gather(gate_w, "tp", axis=2, tiled=True)[0]
    up_piece = lax.all_gather(up_w, "tp", axis=2, tiled=True)[0]
    down_piece = lax.all_gather(down_w, "tp", axis=2, tiled=True)[0]
    produced = expert_rows(slot_rows, gate_piece, up_piece, down_piece)
    results = produced.astype(BF16).reshape(sources, items, width)
    answered = lax.all_to_all(results, sp, split_axis=0, concat_axis=0, tiled=True)
    flat_answers = answered.reshape(experts_all * capacity, normed.shape[1])
    per_route = jnp.einsum("rks,sd->rkd", selector, flat_answers, preferred_element_type=F32)
    return jnp.sum(per_route * weight[:, :, None], axis=1)


def body(
    residual,
    query_values,
    forget_preact,
    value_written,
    output_gate_preact,
    forget_margin,
    sudden_decay,
    head_norm_gain,
    output_weight_matrix,
    mixer_norm_gain,
    feedforward_gain,
    routed_expert_index,
    routed_expert_weight,
    expert_gate_matrix,
    expert_up_matrix,
    expert_down_matrix,
    common_gate_matrix,
    common_up_matrix,
    common_down_matrix,
    final_norm_gain,
    *,
    sp,
):
    tokens, channels = query_values.shape
    rows = residual.shape[0]
    peers = lax.axis_size("tp")
    paired = len(sp) == 2
    if paired:
        outer, inner = sp
        packed = pack_call(expert_gate_matrix, expert_up_matrix, expert_down_matrix)
        held = lax.all_gather(packed, (inner, "tp"))
        held = held.reshape((lax.axis_size(inner), peers) + packed.shape)
        experts_all = lax.axis_size(outer) * lax.axis_size(inner)
        share = jnp.stack(
            [
                jnp.sum(jnp.where(routed_expert_index == e, routed_expert_weight, 0.0), axis=1)
                for e in range(experts_all)
            ]
        )
        pair = lax.axis_size(inner)
        swap = [(0, 1), (1, 0)]
        here = lax.axis_index(outer) == 0
        filler = jnp.zeros((8 - pair, rows), F32)
        own_share = jnp.concatenate([jnp.where(here, share[:pair], share[pair:]), filler])
        far_share = jnp.concatenate([jnp.where(here, share[pair:], share[:pair]), filler])
        far_share = lax.ppermute(far_share, outer, swap)

    local, lifted, final = scan_call(
        query_values, forget_preact, value_written, forget_margin, sudden_decay
    )
    pieces = lax.all_gather(final, sp)
    mine = lax.axis_index(sp).reshape(1)
    gain = jnp.tile(head_norm_gain, channels // HEAD_CHANNELS).reshape(1, channels)
    mixed = gate_call(mine, local, lifted, output_gate_preact, pieces, gain)
    mixed = lax.all_to_all(
        mixed.reshape(peers, tokens // peers, channels), "tp", split_axis=0, concat_axis=0, tiled=True
    )
    if channels % 128 == 0:
        stream, normed, shared = project_call(
            mixed,
            output_weight_matrix,
            residual,
            mixer_norm_gain,
            feedforward_gain,
            (common_gate_matrix, common_up_matrix, common_down_matrix),
        )
    else:
        mixed = mixed.transpose(1, 0, 2).reshape(rows, peers * channels)
        projected = jnp.dot(mixed, output_weight_matrix, preferred_element_type=F32).astype(BF16)
        stream = (residual.astype(F32) + rms_scale(projected.astype(F32)) * mixer_norm_gain).astype(BF16)
        normed = (rms_scale(stream.astype(F32)) * feedforward_gain).astype(BF16)
        shared = shared_expert(normed, common_gate_matrix, common_up_matrix, common_down_matrix)
    if not paired:
        routed = routed_by_slots(
            normed,
            routed_expert_index,
            routed_expert_weight,
            expert_gate_matrix,
            expert_up_matrix,
            expert_down_matrix,
            sp,
        )
        layer_out = stream.astype(F32) + rms_scale(shared + routed) * final_norm_gain
        return layer_out.astype(BF16)
    first = 3 * rows // 8
    far_first = lax.ppermute(normed[:first], outer, swap)
    far_rest = lax.ppermute(normed[first:], outer, swap)
    (partial,) = expert_call(far_first, far_share[:, :first], held, None, (first,), BF16, "far0", 4)
    answers = [lax.ppermute(partial, outer, swap)]
    far_rest, _ = lax.optimization_barrier((far_rest, partial))
    sizes = (rows - 2 * first, first)
    partials = expert_call(far_rest, far_share[:, first:], held, None, sizes, BF16, "far1", 4)
    answers += [lax.ppermute(partial, outer, swap) for partial in partials]
    own_rows, _ = lax.optimization_barrier((normed, partials[1]))
    (base,) = expert_call(own_rows, own_share, held, shared, (rows,), F32, "own", 2)
    layer_out = None
    starts = (0, first, first + sizes[0])
    for c in (0, 2, 1):
        layer_out = combine_call(layer_out, stream, base, answers[c], final_norm_gain, starts[c])
    return layer_out


def solution(mesh):
    sp_size, tp_size = mesh.shape["sp"], mesh.shape["tp"]
    if sp_size == 4:
        sp = ("far", "near")
        mesh = Mesh(mesh.devices.reshape(2, 2, tp_size), sp + ("tp",))
    else:
        sp = ("sp",)
    every = P(sp + ("tp",), None)
    split = P(sp, "tp")
    shard = P(sp, None, "tp")
    placed = (
        every,
        split,
        split,
        split,
        split,
        P("tp"),
        P("tp", sp),
        P(),
        P(),
        P(),
        P(),
        every,
        every,
        shard,
        shard,
        shard,
        P(),
        P(),
        P(),
        P(),
    )
    return jax.shard_map(
        functools.partial(body, sp=sp), mesh=mesh, in_specs=placed, out_specs=every, check_vma=False
    )
```

```python
import functools

import jax
import jax.numpy as jnp
from jax import lax
from jax.experimental import pallas as pl
from jax.experimental.pallas import tpu as pltpu
from jax.sharding import Mesh, PartitionSpec as P


HEAD_CHANNELS = 64
BLOCK = 64
EPS = 1e-06
TOP_PRECISION = lax.Precision.HIGHEST
F32 = jnp.float32
BF16 = jnp.bfloat16

LANES_LANES = (((1,), (1,)), ((), ()))
ROWS_ROWS = (((0,), (0,)), ((), ()))


def rms_scale(values):
    return values * lax.rsqrt(jnp.mean(values * values, axis=-1, keepdims=True) + EPS)


def mm(a, b, dims=(((1,), (0,)), ((), ()))):
    return lax.dot_general(a, b, dims, preferred_element_type=F32)


def halves(value):
    top = value.astype(BF16)
    return top, (value - top.astype(F32)).astype(BF16)


def fine_mm(a, b):
    a_top, a_rest = a
    b_top, b_rest = b
    return mm(
        jnp.concatenate([a_top, a_rest, a_top], axis=1),
        jnp.concatenate([b_top, b_top, b_rest], axis=1),
        LANES_LANES,
    )


def scan_kernel(
    q_ref, f_ref, v_ref, margin_ref, sudden_ref, local_ref, lifted_ref, final_ref, state_ref, total_ref
):
    step = pl.program_id(0)
    span, channels = q_ref.shape
    heads = channels // HEAD_CHANNELS

    @pl.when(step == 0)
    def _():
        state_ref[...] = jnp.zeros_like(state_ref)
        total_ref[...] = jnp.zeros_like(total_ref)

    lane = lax.broadcasted_iota(jnp.int32, (BLOCK, channels), 1) // HEAD_CHANNELS

    def per_head(block):
        if heads == 1:
            return block
        return jnp.concatenate(
            [jnp.where(lane == h, block, jnp.zeros_like(block)) for h in range(heads)], axis=0
        )

    rows = lax.broadcasted_iota(jnp.int32, (BLOCK, heads * BLOCK), 0)
    cols = lax.broadcasted_iota(jnp.int32, (BLOCK, heads * BLOCK), 1) % BLOCK
    lower = rows >= cols
    sum_rows = lax.broadcasted_iota(jnp.int32, (BLOCK, 3 * BLOCK), 0)
    sum_cols = lax.broadcasted_iota(jnp.int32, (BLOCK, 3 * BLOCK), 1) % BLOCK
    summing = (sum_rows >= sum_cols).astype(F32).astype(BF16)
    own_head = (
        lax.broadcasted_iota(jnp.int32, (channels, channels), 0) // HEAD_CHANNELS
        == lax.broadcasted_iota(jnp.int32, (channels, channels), 1) // HEAD_CHANNELS
    )
    margin = margin_ref[...]
    sudden = sudden_ref[...]
    sudden = jnp.concatenate([sudden, jnp.zeros((8 - heads, span), F32)], axis=0).T
    state = state_ref[...]
    total = total_ref[...]
    for j in range(span // BLOCK):
        at = pl.ds(j * BLOCK, BLOCK)
        strength = margin * jax.nn.sigmoid(-f_ref[at, :].astype(F32))
        extra = sudden[j * BLOCK : (j + 1) * BLOCK]
        jump = jnp.broadcast_to(extra[:, 0:1], (BLOCK, channels))
        for h in range(1, heads):
            jump = jnp.where(lane == h, jnp.broadcast_to(extra[:, h : h + 1], (BLOCK, channels)), jump)
        keep = jnp.log1p(-strength) + jump
        top = keep.astype(BF16)
        rest = keep - top.astype(F32)
        second = rest.astype(BF16)
        third = (rest - second.astype(F32)).astype(BF16)
        running = mm(summing, jnp.concatenate([top, second, third], axis=0))
        middle = running[BLOCK // 2 - 1 : BLOCK // 2]
        closing = running[BLOCK - 1 : BLOCK]
        scaled_q = q_ref[at, :].astype(F32) * jnp.exp(running - middle)
        scaled_k = strength * jnp.exp(middle - running)
        values = v_ref[at, :]
        k_top, k_rest = halves(scaled_k)
        scores = fine_mm(halves(scaled_q), (per_head(k_top), per_head(k_rest)))
        score_top, score_rest = halves(jnp.where(lower, scores, 0.0))
        spread = per_head(values)
        lifted = scaled_q * jnp.exp(middle)
        local_ref[at, :] = mm(
            jnp.concatenate([score_top, score_rest], axis=1), jnp.concatenate([spread, spread], axis=0)
        ) + fine_mm(halves(lifted), halves(state))
        lifted_ref[at, :] = lifted * jnp.exp(total)
        closed_k = jnp.concatenate(halves(scaled_k * jnp.exp(closing - middle)), axis=0)
        added = mm(jnp.concatenate([values, values], axis=0), closed_k, ROWS_ROWS)
        state = state * jnp.exp(closing) + jnp.where(own_head, added, 0.0)
        total = total + closing
    state_ref[...] = state
    total_ref[...] = total
    final_ref[0:channels, :] = state
    final_ref[channels:, :] = jnp.broadcast_to(jnp.exp(total), (8, channels))


def scan_call(q, f, v, margin, sudden):
    tokens, channels = q.shape
    heads = channels // HEAD_CHANNELS
    span = min(tokens, 512)
    block = pl.BlockSpec((span, channels), lambda i: (i, 0))
    return pl.pallas_call(
        scan_kernel,
        grid=(tokens // span,),
        in_specs=[
            block,
            block,
            block,
            pl.BlockSpec((1, channels), lambda i: (0, 0)),
            pl.BlockSpec((heads, span), lambda i: (0, i)),
        ],
        out_specs=[block, block, pl.BlockSpec((channels + 8, channels), lambda i: (0, 0))],
        out_shape=[
            jax.ShapeDtypeStruct((tokens, channels), F32),
            jax.ShapeDtypeStruct((tokens, channels), F32),
            jax.ShapeDtypeStruct((channels + 8, channels), F32),
        ],
        scratch_shapes=[pltpu.VMEM((channels, channels), F32), pltpu.VMEM((1, channels), F32)],
        compiler_params=pltpu.CompilerParams(dimension_semantics=("arbitrary",)),
        cost_estimate=pl.CostEstimate(
            flops=tokens * channels * 2000, bytes_accessed=tokens * channels * 14, transcendentals=0
        ),
        name="scan",
    )(q, f, v, margin.reshape(1, channels), sudden)


def gate_kernel(mine_ref, local_ref, lifted_ref, open_ref, pieces_ref, gain_ref, mixed_ref):
    _, channels = local_ref.shape
    mine = mine_ref[0]
    incoming = jnp.zeros((channels, channels), F32)
    for j in range(pieces_ref.shape[0] - 1):
        at = mine_ref[1 + j]
        longer = incoming * pieces_ref[at, channels : channels + 1, :] + pieces_ref[at, 0:channels, :]
        incoming = jnp.where(j < mine, longer, incoming)
    heads_out = local_ref[...] + fine_mm(halves(lifted_ref[...]), halves(incoming))
    own_head = (
        lax.broadcasted_iota(jnp.int32, (channels, channels), 0) // HEAD_CHANNELS
        == lax.broadcasted_iota(jnp.int32, (channels, channels), 1) // HEAD_CHANNELS
    )
    averaging = jnp.where(own_head, 1.0 / HEAD_CHANNELS, 0.0).astype(BF16)
    square = heads_out * heads_out
    top = square.astype(BF16)
    rest = (square - top.astype(F32)).astype(BF16)
    mean = mm(top, averaging) + mm(rest, averaging)
    opening = jax.nn.sigmoid(open_ref[...].astype(F32))
    mixed_ref[...] = (heads_out * lax.rsqrt(mean + EPS) * gain_ref[...] * opening).astype(BF16)


def gate_call(mine, local, lifted, opening, pieces, gain):
    tokens, channels = local.shape
    span = min(tokens, 1024)
    block = pl.BlockSpec((span, channels), lambda i: (i, 0))
    return pl.pallas_call(
        gate_kernel,
        grid=(tokens // span,),
        in_specs=[
            pl.BlockSpec(memory_space=pltpu.SMEM),
            block,
            block,
            block,
            pl.BlockSpec(pieces.shape, lambda i: (0, 0, 0)),
            pl.BlockSpec((1, channels), lambda i: (0, 0)),
        ],
        out_specs=block,
        out_shape=jax.ShapeDtypeStruct((tokens, channels), BF16),
        compiler_params=pltpu.CompilerParams(dimension_semantics=("arbitrary",)),
        cost_estimate=pl.CostEstimate(
            flops=tokens * channels * 800, bytes_accessed=tokens * channels * 10, transcendentals=0
        ),
        name="gate",
    )(mine, local, lifted, opening, pieces, gain)


def project_kernel(
    mixed_ref,
    weight_ref,
    residual_ref,
    mixer_ref,
    gain_ref,
    gate_ref,
    up_ref,
    down_ref,
    stream_ref,
    normed_ref,
    shared_ref,
):
    mixed = jnp.concatenate([mixed_ref[j] for j in range(mixed_ref.shape[0])], axis=1)
    projected = mm(mixed, weight_ref[...]).astype(BF16).astype(F32)
    stream = (residual_ref[...].astype(F32) + rms_scale(projected) * mixer_ref[...]).astype(BF16)
    stream_ref[...] = stream
    normed = (rms_scale(stream.astype(F32)) * gain_ref[...]).astype(BF16)
    normed_ref[...] = normed
    gate = mm(normed, gate_ref[...])
    hidden = (gate * jax.nn.sigmoid(gate) * mm(normed, up_ref[...])).astype(BF16)
    shared_ref[...] = mm(hidden, down_ref[...])


def project_call(mixed, weight, residual, mixer_gain, gain, shared_weights):
    sources, rows, channels = mixed.shape
    width = weight.shape[1]
    span = min(rows, 256)
    block = pl.BlockSpec((span, width), lambda i: (i, 0))

    def whole(array):
        return pl.BlockSpec(array.shape, lambda i: (0, 0))

    vectors = [mixer_gain.reshape(1, width), gain.reshape(1, width)]
    hidden = shared_weights[0].shape[1]
    return pl.pallas_call(
        project_kernel,
        grid=(rows // span,),
        in_specs=[pl.BlockSpec((sources, span, channels), lambda i: (0, i, 0)), whole(weight), block]
        + [whole(array) for array in vectors + list(shared_weights)],
        out_specs=[block, block, block],
        out_shape=[
            jax.ShapeDtypeStruct((rows, width), BF16),
            jax.ShapeDtypeStruct((rows, width), BF16),
            jax.ShapeDtypeStruct((rows, width), F32),
        ],
        compiler_params=pltpu.CompilerParams(
            dimension_semantics=("arbitrary",), vmem_limit_bytes=48 * 1024 * 1024
        ),
        cost_estimate=pl.CostEstimate(
            flops=2 * rows * width * (weight.shape[0] + 3 * hidden),
            bytes_accessed=2 * weight.size + 12 * rows * width,
            transcendentals=0,
        ),
        name="project",
    )(mixed, weight, residual, *vectors, *shared_weights)


def pack_kernel(gate_ref, up_ref, down_ref, upper_ref, lower_ref):
    width, units = gate_ref.shape[1:]
    half = upper_ref.shape[0]
    upper_ref[:, 0:units] = gate_ref[0, 0:half, :]
    upper_ref[:, units:] = up_ref[0, 0:half, :]
    lower_ref[0 : width - half, 0:units] = gate_ref[0, half:, :]
    lower_ref[0 : width - half, units:] = up_ref[0, half:, :]
    for j in range(width // (2 * units)):
        turned = down_ref[0, j * 2 * units : (j + 1) * 2 * units, :].T
        lower_ref[width - half + j * units : width - half + (j + 1) * units, :] = turned


def pack_call(gate, up, down):
    _, width, units = gate.shape
    return pl.pallas_call(
        pack_kernel,
        out_shape=[jax.ShapeDtypeStruct((3 * width // 4, 2 * units), gate.dtype)] * 2,
        cost_estimate=pl.CostEstimate(flops=0, bytes_accessed=12 * width * units, transcendentals=0),
        name="pack",
    )(gate, up, down)


def expert_kernel(*refs, based, sources):
    which_ref, rows_ref, share_ref = refs[:3]
    piece_refs = refs[3 + based : 3 + based + len(sources)]
    out_refs = refs[3 + based + len(sources) : -4]
    held_ref, sum_ref, wide_ref, sems = refs[-4:]
    width = rows_ref.shape[1]
    pieces, _, double = held_ref.shape
    units = double // 2
    for ref, (slot, start) in zip(piece_refs, sources):
        into = held_ref.at[slot, start : start + ref.shape[0]]
        pltpu.make_async_copy(ref, into, sems.at[slot]).start()
    sum_ref[...] = jnp.zeros_like(sum_ref)
    share = share_ref[...].T
    for e in range(wide_ref.shape[0]):
        wide_ref[e] = jnp.broadcast_to(share[:, e : e + 1], wide_ref.shape[1:])

    for g in range(pieces // TOGETHER):
        slots = range(g * TOGETHER, (g + 1) * TOGETHER)
        for slot in slots:
            pltpu.make_async_copy(held_ref.at[slot], held_ref.at[slot], sems.at[slot]).wait()
        hidden = []
        for slot in slots:
            part = wide_ref[which_ref[slot]]
            both = mm(rows_ref[...], held_ref[slot, 0:width, :])
            gate, up = both[:, :units], both[:, units:]
            hidden.append((gate * jax.nn.sigmoid(gate) * up * part).astype(BF16))
        hidden = jnp.concatenate(hidden, axis=1)
        for c in range(width // double):
            at = slice(width + c * units, width + (c + 1) * units)
            down = jnp.concatenate([held_ref[slot, at, :] for slot in slots], axis=0)
            sum_ref[:, c * double : (c + 1) * double] += mm(hidden, down)
    start = 0
    for out_ref in out_refs:
        at = slice(start, start + out_ref.shape[0])
        total = sum_ref[at, :] + refs[3][at, :] if based else sum_ref[at, :]
        out_ref[...] = total.astype(out_ref.dtype)
        start += out_ref.shape[0]


TOGETHER = 2


def expert_call(which, rows, share, held, base, sizes, kind):
    count, width = rows.shape
    arrays = [array for array, _, _ in held]
    sources = [(slot, start) for _, slot, start in held]
    double = arrays[0].shape[1]
    depth = width + width // 2
    pieces = 1 + max(slot for slot, _ in sources)
    specs = [pl.BlockSpec(memory_space=pltpu.SMEM)] + [pl.BlockSpec(memory_space=pltpu.VMEM)] * 2
    operands = [which, rows, share]
    if base is not None:
        specs.append(pl.BlockSpec(memory_space=pltpu.VMEM))
        operands.append(base)
    specs += [pl.BlockSpec(memory_space=pltpu.HBM)] * len(arrays)
    return pl.pallas_call(
        functools.partial(expert_kernel, based=base is not None, sources=sources),
        in_specs=specs,
        out_specs=[pl.BlockSpec(memory_space=pltpu.VMEM)] * len(sizes),
        out_shape=[jax.ShapeDtypeStruct((size, width), kind) for size in sizes],
        scratch_shapes=[
            pltpu.VMEM((pieces, depth, double), BF16),
            pltpu.VMEM((count, width), F32),
            pltpu.VMEM((2, count, double // 2), F32),
            pltpu.SemaphoreType.DMA((pieces,)),
        ],
        compiler_params=pltpu.CompilerParams(vmem_limit_bytes=60 * 1024 * 1024),
        cost_estimate=pl.CostEstimate(
            flops=2 * count * pieces * depth * double,
            bytes_accessed=2 * pieces * depth * double,
            transcendentals=0,
        ),
    )(*operands, *arrays)


def ring_hops(columns, peers):
    long = peers // 2
    size = columns * long

    def device(r, core):
        column, level = (0, r) if r < long else (1, size - 1 - r)
        return column * peers + level * 2 + core

    def shift(by):
        return [(device(r, c), device((r + by) % size, c)) for r in range(size) for c in (0, 1)]

    swap = [(z * 2 + c, z * 2 + 1 - c) for z in range(long) for c in (0, 1)]
    return shift(1), shift(-1), swap


def combine_kernel(*refs):
    stream_ref, base_ref, answer_ref, gain_ref, out_ref = refs[-5:]
    summed = base_ref[...] + answer_ref[...].astype(F32)
    out_ref[...] = (stream_ref[...].astype(F32) + rms_scale(summed) * gain_ref[...]).astype(BF16)


def combine_call(so_far, stream, base, answer, gain, start):
    rows, width = stream.shape
    span = min(answer.shape[0], 64)
    skip = start // span
    block = pl.BlockSpec((span, width), lambda i: (skip + i, 0))
    specs = [block, block, pl.BlockSpec((span, width), lambda i: (i, 0))]
    specs.append(pl.BlockSpec((1, width), lambda i: (0, 0)))
    operands = [stream, base, answer, gain.reshape(1, width)]
    aliases = {}
    if so_far is not None:
        specs.insert(0, pl.BlockSpec(memory_space=pl.ANY))
        operands.insert(0, so_far)
        aliases = {0: 0}
    return pl.pallas_call(
        combine_kernel,
        grid=(answer.shape[0] // span,),
        in_specs=specs,
        out_specs=block,
        out_shape=jax.ShapeDtypeStruct((rows, width), BF16),
        input_output_aliases=aliases,
        compiler_params=pltpu.CompilerParams(dimension_semantics=("arbitrary",)),
        cost_estimate=pl.CostEstimate(
            flops=answer.size, bytes_accessed=10 * answer.size, transcendentals=0
        ),
    )(*operands)


def shared_expert(normed, gate_w, up_w, down_w):
    hidden = (
        jax.nn.silu(jnp.dot(normed, gate_w, preferred_element_type=F32))
        * jnp.dot(normed, up_w, preferred_element_type=F32)
    ).astype(BF16)
    return jnp.dot(hidden, down_w, preferred_element_type=F32)


def expert_rows(slot_rows, gate_w, up_w, down_w):
    hidden = (
        jax.nn.silu(jnp.dot(slot_rows, gate_w, preferred_element_type=F32))
        * jnp.dot(slot_rows, up_w, preferred_element_type=F32)
    ).astype(BF16)
    return lax.dot_general(hidden, down_w, LANES_LANES, preferred_element_type=F32)


def routed_by_slots(normed, index, weight, gate_w, up_w, down_w, sp):
    rows_here, routes_each = index.shape
    experts_all = lax.axis_size(sp)
    capacity = 3 * rows_here * routes_each // (2 * experts_all)
    numbers = jnp.arange(experts_all, dtype=jnp.int32)
    matches = (index[:, :, None] == numbers).astype(F32)
    hits = jnp.sum(matches, axis=1)
    strictly_lower = jnp.tril(jnp.ones((rows_here, rows_here), F32), -1)
    before_hits = jnp.dot(strictly_lower, hits, precision=TOP_PRECISION)
    slots = jnp.sum(before_hits[:, None, :] * matches, axis=2).astype(jnp.int32)
    targets = index * capacity + slots
    slot_numbers = jnp.arange(experts_all * capacity, dtype=jnp.int32)
    selector = (targets[:, :, None] == slot_numbers).astype(BF16)
    outgoing = jnp.einsum("rks,rd->sd", selector, normed, preferred_element_type=F32)
    outgoing = outgoing.astype(BF16).reshape(experts_all, capacity, normed.shape[1])
    arrived = lax.all_to_all(outgoing, sp, split_axis=0, concat_axis=0, tiled=True)
    sources, items, width = arrived.shape
    slot_rows = arrived.reshape(sources * items, width)
    gate_piece = lax.all_gather(gate_w, "tp", axis=2, tiled=True)[0]
    up_piece = lax.all_gather(up_w, "tp", axis=2, tiled=True)[0]
    down_piece = lax.all_gather(down_w, "tp", axis=2, tiled=True)[0]
    produced = expert_rows(slot_rows, gate_piece, up_piece, down_piece)
    results = produced.astype(BF16).reshape(sources, items, width)
    answered = lax.all_to_all(results, sp, split_axis=0, concat_axis=0, tiled=True)
    flat_answers = answered.reshape(experts_all * capacity, normed.shape[1])
    per_route = jnp.einsum("rks,sd->rkd", selector, flat_answers, preferred_element_type=F32)
    return jnp.sum(per_route * weight[:, :, None], axis=1)


def body(
    residual,
    query_values,
    forget_preact,
    value_written,
    output_gate_preact,
    forget_margin,
    sudden_decay,
    head_norm_gain,
    output_weight_matrix,
    mixer_norm_gain,
    feedforward_gain,
    routed_expert_index,
    routed_expert_weight,
    expert_gate_matrix,
    expert_up_matrix,
    expert_down_matrix,
    common_gate_matrix,
    common_up_matrix,
    common_down_matrix,
    final_norm_gain,
    *,
    sp,
):
    tokens, channels = query_values.shape
    rows = residual.shape[0]
    peers = lax.axis_size("tp")
    paired = len(sp) == 2
    if paired:
        outer, inner = sp
        ring = (inner, "tp")
        forward, backward, partner = ring_hops(lax.axis_size(inner), peers)
        upper, lower = pack_call(expert_gate_matrix, expert_up_matrix, expert_down_matrix)
        hops = {"long": ([upper], [lower]), "short": ([lower], [upper])}

        def hop(kind):
            for perm, chain in zip((forward, backward), hops[kind]):
                chain.append(lax.ppermute(chain[-1], ring, perm))

        hop("long")
        hop("short")
        level = lax.axis_index("tp") // 2
        size = peers
        place = jnp.where(lax.axis_index(inner) == 0, level, size - 1 - level)
        origin = [place, place]
        for k in range(1, size // 2):
            origin += [place - k, place - k, place + k, place + k]
        origin += [place + size // 2] * 2
        which = ((jnp.stack(origin) % size) >= size // 2).astype(jnp.int32)
        experts_all = lax.axis_size(outer) * lax.axis_size(inner)
        share = jnp.stack(
            [
                jnp.sum(jnp.where(routed_expert_index == e, routed_expert_weight, 0.0), axis=1)
                for e in range(experts_all)
            ]
        )
        pair = lax.axis_size(inner)
        swap = [(0, 1), (1, 0)]
        here = lax.axis_index(outer) == 0
        filler = jnp.zeros((8 - pair, rows), F32)
        own_share = jnp.concatenate([jnp.where(here, share[:pair], share[pair:]), filler])
        far_share = jnp.concatenate([jnp.where(here, share[pair:], share[:pair]), filler])
        far_share = lax.ppermute(far_share, outer, swap)

    local, lifted, final = scan_call(
        query_values, forget_preact, value_written, forget_margin, sudden_decay
    )
    mine = lax.axis_index(sp)
    if paired:
        others = [
            lax.ppermute(final, sp, [(i, i ^ other) for i in range(4)]) for other in (1, 2, 3)
        ]
        pieces = jnp.stack([final] + others)
        order = mine ^ jnp.arange(4)
        hop("long")
        hop("short")
    else:
        pieces = lax.all_gather(final, sp)
        order = jnp.arange(pieces.shape[0])
    mine = jnp.concatenate([mine.reshape(1), order])
    gain = jnp.tile(head_norm_gain, channels // HEAD_CHANNELS).reshape(1, channels)
    mixed = gate_call(mine, local, lifted, output_gate_preact, pieces, gain)
    mixed = lax.all_to_all(
        mixed.reshape(peers, tokens // peers, channels), "tp", split_axis=0, concat_axis=0, tiled=True
    )
    if paired:
        hop("long")
        hop("short")
    if channels % 128 == 0:
        stream, normed, shared = project_call(
            mixed,
            output_weight_matrix,
            residual,
            mixer_norm_gain,
            feedforward_gain,
            (common_gate_matrix, common_up_matrix, common_down_matrix),
        )
    else:
        mixed = mixed.transpose(1, 0, 2).reshape(rows, peers * channels)
        projected = jnp.dot(mixed, output_weight_matrix, preferred_element_type=F32).astype(BF16)
        stream = (residual.astype(F32) + rms_scale(projected.astype(F32)) * mixer_norm_gain).astype(BF16)
        normed = (rms_scale(stream.astype(F32)) * feedforward_gain).astype(BF16)
        shared = shared_expert(normed, common_gate_matrix, common_up_matrix, common_down_matrix)
    if not paired:
        routed = routed_by_slots(
            normed,
            routed_expert_index,
            routed_expert_weight,
            expert_gate_matrix,
            expert_up_matrix,
            expert_down_matrix,
            sp,
        )
        layer_out = stream.astype(F32) + rms_scale(shared + routed) * final_norm_gain
        return layer_out.astype(BF16)
    first = 3 * rows // 8
    far_first = lax.ppermute(normed[:first], outer, swap)
    far_rest = lax.ppermute(normed[first:], outer, swap)
    hop("long")

    held = []

    def hold(slot, start, array):
        held.append((array, slot, start))
        held.append((lax.ppermute(array, "tp", partner), slot + 1, start))

    half = upper.shape[0]
    (long_a, long_b), (short_a, short_b) = hops["long"], hops["short"]
    hold(0, 0, upper)
    hold(0, half, lower)
    for k in range(1, 4):
        hold(4 * k - 2, 0, long_a[k])
        hold(4 * k - 2, half, short_a[k])
        hold(4 * k, 0, short_b[k])
        hold(4 * k, half, long_b[k])
    hold(14, 0, long_a[4])
    hold(14, half, long_b[4])
    (partial,) = expert_call(which, far_first, far_share[:, :first], held, None, (first,), BF16)
    answers = [lax.ppermute(partial, outer, swap)]
    far_rest, _ = lax.optimization_barrier((far_rest, partial))
    sizes = (rows - 2 * first, first)
    partials = expert_call(which, far_rest, far_share[:, first:], held, None, sizes, BF16)
    answers += [lax.ppermute(partial, outer, swap) for partial in partials]
    own_rows, _ = lax.optimization_barrier((normed, partials[1]))
    (base,) = expert_call(which, own_rows, own_share, held, shared, (rows,), F32)
    layer_out = None
    starts = (0, first, first + sizes[0])
    for c in (0, 2, 1):
        layer_out = combine_call(layer_out, stream, base, answers[c], final_norm_gain, starts[c])
    return layer_out


def solution(mesh):
    sp_size, tp_size = mesh.shape["sp"], mesh.shape["tp"]
    if sp_size == 4:
        sp = ("far", "near")
        mesh = Mesh(mesh.devices.reshape(2, 2, tp_size), sp + ("tp",))
    else:
        sp = ("sp",)
    every = P(sp + ("tp",), None)
    split = P(sp, "tp")
    shard = P(sp, None, "tp")
    placed = (
        every,
        split,
        split,
        split,
        split,
        P("tp"),
        P("tp", sp),
        P(),
        P(),
        P(),
        P(),
        every,
        every,
        shard,
        shard,
        shard,
        P(),
        P(),
        P(),
        P(),
    )

    def step(*arrays):
        return body(*arrays, sp=sp)

    return jax.shard_map(step, mesh=mesh, in_specs=placed, out_specs=every, check_vma=False)
```

```python
import functools

import jax
import jax.numpy as jnp
from jax import lax
from jax.experimental import pallas as pl
from jax.experimental.pallas import tpu as pltpu
from jax.sharding import Mesh, PartitionSpec as P


HEAD_CHANNELS = 64
BLOCK = 64
EPS = 1e-06
TOP_PRECISION = lax.Precision.HIGHEST
F32 = jnp.float32
BF16 = jnp.bfloat16

LANES_LANES = (((1,), (1,)), ((), ()))
ROWS_ROWS = (((0,), (0,)), ((), ()))


def rms_scale(values):
    return values * lax.rsqrt(jnp.mean(values * values, axis=-1, keepdims=True) + EPS)


def mm(a, b, dims=(((1,), (0,)), ((), ()))):
    return lax.dot_general(a, b, dims, preferred_element_type=F32)


def halves(value):
    top = value.astype(BF16)
    return top, (value - top.astype(F32)).astype(BF16)


def fine_mm(a, b):
    a_top, a_rest = a
    b_top, b_rest = b
    return mm(
        jnp.concatenate([a_top, a_rest, a_top], axis=1),
        jnp.concatenate([b_top, b_top, b_rest], axis=1),
        LANES_LANES,
    )


def scan_kernel(
    q_ref, f_ref, v_ref, margin_ref, sudden_ref, local_ref, lifted_ref, final_ref, state_ref, total_ref
):
    step = pl.program_id(0)
    span, channels = q_ref.shape
    heads = channels // HEAD_CHANNELS

    @pl.when(step == 0)
    def _():
        state_ref[...] = jnp.zeros_like(state_ref)
        total_ref[...] = jnp.zeros_like(total_ref)

    lane = lax.broadcasted_iota(jnp.int32, (BLOCK, channels), 1) // HEAD_CHANNELS

    def per_head(block):
        if heads == 1:
            return block
        return jnp.concatenate(
            [jnp.where(lane == h, block, jnp.zeros_like(block)) for h in range(heads)], axis=0
        )

    rows = lax.broadcasted_iota(jnp.int32, (BLOCK, heads * BLOCK), 0)
    cols = lax.broadcasted_iota(jnp.int32, (BLOCK, heads * BLOCK), 1) % BLOCK
    lower = rows >= cols
    sum_rows = lax.broadcasted_iota(jnp.int32, (BLOCK, 3 * BLOCK), 0)
    sum_cols = lax.broadcasted_iota(jnp.int32, (BLOCK, 3 * BLOCK), 1) % BLOCK
    summing = (sum_rows >= sum_cols).astype(F32).astype(BF16)
    own_head = (
        lax.broadcasted_iota(jnp.int32, (channels, channels), 0) // HEAD_CHANNELS
        == lax.broadcasted_iota(jnp.int32, (channels, channels), 1) // HEAD_CHANNELS
    )
    margin = margin_ref[...]
    sudden = sudden_ref[...]
    sudden = jnp.concatenate([sudden, jnp.zeros((8 - heads, span), F32)], axis=0).T
    state = state_ref[...]
    total = total_ref[...]
    for j in range(span // BLOCK):
        at = pl.ds(j * BLOCK, BLOCK)
        strength = margin * jax.nn.sigmoid(-f_ref[at, :].astype(F32))
        extra = sudden[j * BLOCK : (j + 1) * BLOCK]
        jump = jnp.broadcast_to(extra[:, 0:1], (BLOCK, channels))
        for h in range(1, heads):
            jump = jnp.where(lane == h, jnp.broadcast_to(extra[:, h : h + 1], (BLOCK, channels)), jump)
        keep = jnp.log1p(-strength) + jump
        top = keep.astype(BF16)
        rest = keep - top.astype(F32)
        second = rest.astype(BF16)
        third = (rest - second.astype(F32)).astype(BF16)
        running = mm(summing, jnp.concatenate([top, second, third], axis=0))
        middle = running[BLOCK // 2 - 1 : BLOCK // 2]
        closing = running[BLOCK - 1 : BLOCK]
        scaled_q = q_ref[at, :].astype(F32) * jnp.exp(running - middle)
        scaled_k = strength * jnp.exp(middle - running)
        values = v_ref[at, :]
        k_top, k_rest = halves(scaled_k)
        scores = fine_mm(halves(scaled_q), (per_head(k_top), per_head(k_rest)))
        score_top, score_rest = halves(jnp.where(lower, scores, 0.0))
        spread = per_head(values)
        lifted = scaled_q * jnp.exp(middle)
        local_ref[at, :] = mm(
            jnp.concatenate([score_top, score_rest], axis=1), jnp.concatenate([spread, spread], axis=0)
        ) + fine_mm(halves(lifted), halves(state))
        lifted_ref[at, :] = lifted * jnp.exp(total)
        closed_k = jnp.concatenate(halves(scaled_k * jnp.exp(closing - middle)), axis=0)
        added = mm(jnp.concatenate([values, values], axis=0), closed_k, ROWS_ROWS)
        state = state * jnp.exp(closing) + jnp.where(own_head, added, 0.0)
        total = total + closing
    state_ref[...] = state
    total_ref[...] = total
    final_ref[0:channels, :] = state
    final_ref[channels:, :] = jnp.broadcast_to(jnp.exp(total), (8, channels))


def scan_call(q, f, v, margin, sudden):
    tokens, channels = q.shape
    heads = channels // HEAD_CHANNELS
    span = min(tokens, 512)
    block = pl.BlockSpec((span, channels), lambda i: (i, 0))
    return pl.pallas_call(
        scan_kernel,
        grid=(tokens // span,),
        in_specs=[
            block,
            block,
            block,
            pl.BlockSpec((1, channels), lambda i: (0, 0)),
            pl.BlockSpec((heads, span), lambda i: (0, i)),
        ],
        out_specs=[block, block, pl.BlockSpec((channels + 8, channels), lambda i: (0, 0))],
        out_shape=[
            jax.ShapeDtypeStruct((tokens, channels), F32),
            jax.ShapeDtypeStruct((tokens, channels), F32),
            jax.ShapeDtypeStruct((channels + 8, channels), F32),
        ],
        scratch_shapes=[pltpu.VMEM((channels, channels), F32), pltpu.VMEM((1, channels), F32)],
        compiler_params=pltpu.CompilerParams(dimension_semantics=("arbitrary",)),
        cost_estimate=pl.CostEstimate(
            flops=tokens * channels * 2000, bytes_accessed=tokens * channels * 14, transcendentals=0
        ),
        name="scan",
    )(q, f, v, margin.reshape(1, channels), sudden)


def gate_kernel(mine_ref, local_ref, lifted_ref, open_ref, pieces_ref, gain_ref, mixed_ref):
    _, channels = local_ref.shape
    mine = mine_ref[0]
    incoming = jnp.zeros((channels, channels), F32)
    for j in range(pieces_ref.shape[0] - 1):
        at = mine_ref[1 + j]
        longer = incoming * pieces_ref[at, channels : channels + 1, :] + pieces_ref[at, 0:channels, :]
        incoming = jnp.where(j < mine, longer, incoming)
    heads_out = local_ref[...] + fine_mm(halves(lifted_ref[...]), halves(incoming))
    own_head = (
        lax.broadcasted_iota(jnp.int32, (channels, channels), 0) // HEAD_CHANNELS
        == lax.broadcasted_iota(jnp.int32, (channels, channels), 1) // HEAD_CHANNELS
    )
    averaging = jnp.where(own_head, 1.0 / HEAD_CHANNELS, 0.0).astype(BF16)
    square = heads_out * heads_out
    top = square.astype(BF16)
    rest = (square - top.astype(F32)).astype(BF16)
    mean = mm(top, averaging) + mm(rest, averaging)
    opening = jax.nn.sigmoid(open_ref[...].astype(F32))
    mixed_ref[...] = (heads_out * lax.rsqrt(mean + EPS) * gain_ref[...] * opening).astype(BF16)


def gate_call(mine, local, lifted, opening, pieces, gain):
    tokens, channels = local.shape
    span = min(tokens, 1024)
    block = pl.BlockSpec((span, channels), lambda i: (i, 0))
    return pl.pallas_call(
        gate_kernel,
        grid=(tokens // span,),
        in_specs=[
            pl.BlockSpec(memory_space=pltpu.SMEM),
            block,
            block,
            block,
            pl.BlockSpec(pieces.shape, lambda i: (0, 0, 0)),
            pl.BlockSpec((1, channels), lambda i: (0, 0)),
        ],
        out_specs=block,
        out_shape=jax.ShapeDtypeStruct((tokens, channels), BF16),
        compiler_params=pltpu.CompilerParams(dimension_semantics=("arbitrary",)),
        cost_estimate=pl.CostEstimate(
            flops=tokens * channels * 800, bytes_accessed=tokens * channels * 10, transcendentals=0
        ),
        name="gate",
    )(mine, local, lifted, opening, pieces, gain)


def project_kernel(
    mixed_ref,
    weight_ref,
    residual_ref,
    mixer_ref,
    gain_ref,
    gate_ref,
    up_ref,
    down_ref,
    stream_ref,
    normed_ref,
    shared_ref,
):
    mixed = jnp.concatenate([mixed_ref[j] for j in range(mixed_ref.shape[0])], axis=1)
    projected = mm(mixed, weight_ref[...]).astype(BF16).astype(F32)
    stream = (residual_ref[...].astype(F32) + rms_scale(projected) * mixer_ref[...]).astype(BF16)
    stream_ref[...] = stream
    normed = (rms_scale(stream.astype(F32)) * gain_ref[...]).astype(BF16)
    normed_ref[...] = normed
    gate = mm(normed, gate_ref[...])
    hidden = (gate * jax.nn.sigmoid(gate) * mm(normed, up_ref[...])).astype(BF16)
    shared_ref[...] = mm(hidden, down_ref[...])


def project_call(mixed, weight, residual, mixer_gain, gain, shared_weights):
    sources, rows, channels = mixed.shape
    width = weight.shape[1]
    span = min(rows, 256)
    block = pl.BlockSpec((span, width), lambda i: (i, 0))

    def whole(array):
        return pl.BlockSpec(array.shape, lambda i: (0, 0))

    vectors = [mixer_gain.reshape(1, width), gain.reshape(1, width)]
    hidden = shared_weights[0].shape[1]
    return pl.pallas_call(
        project_kernel,
        grid=(rows // span,),
        in_specs=[pl.BlockSpec((sources, span, channels), lambda i: (0, i, 0)), whole(weight), block]
        + [whole(array) for array in vectors + list(shared_weights)],
        out_specs=[block, block, block],
        out_shape=[
            jax.ShapeDtypeStruct((rows, width), BF16),
            jax.ShapeDtypeStruct((rows, width), BF16),
            jax.ShapeDtypeStruct((rows, width), F32),
        ],
        compiler_params=pltpu.CompilerParams(
            dimension_semantics=("arbitrary",), vmem_limit_bytes=48 * 1024 * 1024
        ),
        cost_estimate=pl.CostEstimate(
            flops=2 * rows * width * (weight.shape[0] + 3 * hidden),
            bytes_accessed=2 * weight.size + 12 * rows * width,
            transcendentals=0,
        ),
        name="project",
    )(mixed, weight, residual, *vectors, *shared_weights)


def pack_kernel(gate_ref, up_ref, down_ref, upper_ref, lower_ref):
    width, units = gate_ref.shape[1:]
    half = upper_ref.shape[0]
    upper_ref[:, 0:units] = gate_ref[0, 0:half, :]
    upper_ref[:, units:] = up_ref[0, 0:half, :]
    lower_ref[0 : width - half, 0:units] = gate_ref[0, half:, :]
    lower_ref[0 : width - half, units:] = up_ref[0, half:, :]
    for j in range(width // (2 * units)):
        turned = down_ref[0, j * 2 * units : (j + 1) * 2 * units, :].T
        lower_ref[width - half + j * units : width - half + (j + 1) * units, :] = turned


def pack_call(gate, up, down):
    _, width, units = gate.shape
    return pl.pallas_call(
        pack_kernel,
        out_shape=[jax.ShapeDtypeStruct((3 * width // 4, 2 * units), gate.dtype)] * 2,
        cost_estimate=pl.CostEstimate(flops=0, bytes_accessed=12 * width * units, transcendentals=0),
        name="pack",
    )(gate, up, down)


def expert_kernel(*refs, based, sources, skip):
    which_ref, rows_ref, share_ref = refs[:3]
    piece_refs = refs[3 + based : 3 + based + len(sources)]
    out_refs = refs[3 + based + len(sources) : -4]
    held_ref, sum_ref, wide_ref, sems = refs[-4:]
    width = rows_ref.shape[1]
    pieces, _, double = held_ref.shape
    units = double // 2
    for ref, (slot, start) in zip(piece_refs, sources):
        into = held_ref.at[slot, start : start + ref.shape[0]]
        pltpu.make_async_copy(ref, into, sems.at[slot]).start()
    sum_ref[...] = jnp.zeros_like(sum_ref)
    share = share_ref[...].T[skip : skip + rows_ref.shape[0]]
    for e in range(wide_ref.shape[0]):
        wide_ref[e] = jnp.broadcast_to(share[:, e : e + 1], wide_ref.shape[1:])

    for g in range(pieces // TOGETHER):
        slots = range(g * TOGETHER, (g + 1) * TOGETHER)
        for slot in slots:
            pltpu.make_async_copy(held_ref.at[slot], held_ref.at[slot], sems.at[slot]).wait()
        hidden = []
        for slot in slots:
            part = wide_ref[which_ref[slot]]
            both = mm(rows_ref[...], held_ref[slot, 0:width, :])
            gate, up = both[:, :units], both[:, units:]
            hidden.append((gate * jax.nn.sigmoid(gate) * up * part).astype(BF16))
        hidden = jnp.concatenate(hidden, axis=1)
        for c in range(width // double):
            at = slice(width + c * units, width + (c + 1) * units)
            down = jnp.concatenate([held_ref[slot, at, :] for slot in slots], axis=0)
            sum_ref[:, c * double : (c + 1) * double] += mm(hidden, down)
    start = 0
    for out_ref in out_refs:
        at = slice(start, start + out_ref.shape[0])
        total = sum_ref[at, :] + refs[3][at, :] if based else sum_ref[at, :]
        out_ref[...] = total.astype(out_ref.dtype)
        start += out_ref.shape[0]


TOGETHER = 2


def expert_call(which, rows, share, held, base, sizes, kind, skip=0):
    count, width = rows.shape
    arrays = [array for array, _, _ in held]
    sources = [(slot, start) for _, slot, start in held]
    double = arrays[0].shape[1]
    depth = width + width // 2
    pieces = 1 + max(slot for slot, _ in sources)
    specs = [pl.BlockSpec(memory_space=pltpu.SMEM)] + [pl.BlockSpec(memory_space=pltpu.VMEM)] * 2
    operands = [which, rows, share]
    if base is not None:
        specs.append(pl.BlockSpec(memory_space=pltpu.VMEM))
        operands.append(base)
    specs += [pl.BlockSpec(memory_space=pltpu.HBM)] * len(arrays)
    return pl.pallas_call(
        functools.partial(expert_kernel, based=base is not None, sources=sources, skip=skip),
        in_specs=specs,
        out_specs=[pl.BlockSpec(memory_space=pltpu.VMEM)] * len(sizes),
        out_shape=[jax.ShapeDtypeStruct((size, width), kind) for size in sizes],
        scratch_shapes=[
            pltpu.VMEM((pieces, depth, double), BF16),
            pltpu.VMEM((count, width), F32),
            pltpu.VMEM((2, count, double // 2), F32),
            pltpu.SemaphoreType.DMA((pieces,)),
        ],
        compiler_params=pltpu.CompilerParams(vmem_limit_bytes=60 * 1024 * 1024),
        cost_estimate=pl.CostEstimate(
            flops=2 * count * pieces * depth * double,
            bytes_accessed=2 * pieces * depth * double,
            transcendentals=0,
        ),
    )(*operands, *arrays)


def ring_hops(columns, peers):
    long = peers // 2
    size = columns * long

    def device(r, core):
        column, level = (0, r) if r < long else (1, size - 1 - r)
        return column * peers + level * 2 + core

    def shift(by):
        return [(device(r, c), device((r + by) % size, c)) for r in range(size) for c in (0, 1)]

    swap = [(z * 2 + c, z * 2 + 1 - c) for z in range(long) for c in (0, 1)]
    return shift(1), shift(-1), swap


def combine_kernel(*refs, counts, followed):
    stream_ref, base_ref = refs[followed : followed + 2]
    answer_refs = refs[followed + 2 : -2]
    gain_ref, out_ref = refs[-2:]
    answer = answer_refs[0][...]
    if len(counts) == 2:
        answer = jnp.where(pl.program_id(0) < counts[0], answer, answer_refs[1][...])
    summed = base_ref[...] + answer.astype(F32)
    out_ref[...] = (stream_ref[...].astype(F32) + rms_scale(summed) * gain_ref[...]).astype(BF16)


def combine_call(so_far, stream, base, answers, gain, starts):
    rows, width = stream.shape
    span = min(answers[0].shape[0], 64)
    counts = [answer.shape[0] // span for answer in answers]
    skips = [start // span for start in starts]

    def place(i):
        if len(counts) == 1:
            return skips[0] + i, 0
        return jnp.where(i < counts[0], skips[0] + i, skips[1] + i - counts[0]), 0

    places = [
        lambda i: (jnp.minimum(i, counts[0] - 1), 0),
        lambda i: (jnp.maximum(i - counts[0], 0), 0),
    ]
    block = pl.BlockSpec((span, width), place)
    specs = [block, block] + [pl.BlockSpec((span, width), at) for at in places[: len(counts)]]
    specs.append(pl.BlockSpec((1, width), lambda i: (0, 0)))
    operands = [stream, base, *answers, gain.reshape(1, width)]
    aliases = {}
    if so_far is not None:
        specs.insert(0, pl.BlockSpec(memory_space=pl.ANY))
        operands.insert(0, so_far)
        aliases = {0: 0}
    return pl.pallas_call(
        functools.partial(combine_kernel, counts=counts, followed=int(so_far is not None)),
        grid=(sum(counts),),
        in_specs=specs,
        out_specs=block,
        out_shape=jax.ShapeDtypeStruct((rows, width), BF16),
        input_output_aliases=aliases,
        compiler_params=pltpu.CompilerParams(dimension_semantics=("arbitrary",)),
        cost_estimate=pl.CostEstimate(
            flops=sum(counts) * span * width,
            bytes_accessed=10 * sum(counts) * span * width,
            transcendentals=0,
        ),
    )(*operands)


def shared_expert(normed, gate_w, up_w, down_w):
    hidden = (
        jax.nn.silu(jnp.dot(normed, gate_w, preferred_element_type=F32))
        * jnp.dot(normed, up_w, preferred_element_type=F32)
    ).astype(BF16)
    return jnp.dot(hidden, down_w, preferred_element_type=F32)


def expert_rows(slot_rows, gate_w, up_w, down_w):
    hidden = (
        jax.nn.silu(jnp.dot(slot_rows, gate_w, preferred_element_type=F32))
        * jnp.dot(slot_rows, up_w, preferred_element_type=F32)
    ).astype(BF16)
    return lax.dot_general(hidden, down_w, LANES_LANES, preferred_element_type=F32)


def routed_by_slots(normed, index, weight, gate_w, up_w, down_w, sp):
    rows_here, routes_each = index.shape
    experts_all = lax.axis_size(sp)
    capacity = 3 * rows_here * routes_each // (2 * experts_all)
    numbers = jnp.arange(experts_all, dtype=jnp.int32)
    matches = (index[:, :, None] == numbers).astype(F32)
    hits = jnp.sum(matches, axis=1)
    strictly_lower = jnp.tril(jnp.ones((rows_here, rows_here), F32), -1)
    before_hits = jnp.dot(strictly_lower, hits, precision=TOP_PRECISION)
    slots = jnp.sum(before_hits[:, None, :] * matches, axis=2).astype(jnp.int32)
    targets = index * capacity + slots
    slot_numbers = jnp.arange(experts_all * capacity, dtype=jnp.int32)
    selector = (targets[:, :, None] == slot_numbers).astype(BF16)
    outgoing = jnp.einsum("rks,rd->sd", selector, normed, preferred_element_type=F32)
    outgoing = outgoing.astype(BF16).reshape(experts_all, capacity, normed.shape[1])
    arrived = lax.all_to_all(outgoing, sp, split_axis=0, concat_axis=0, tiled=True)
    sources, items, width = arrived.shape
    slot_rows = arrived.reshape(sources * items, width)
    gate_piece = lax.all_gather(gate_w, "tp", axis=2, tiled=True)[0]
    up_piece = lax.all_gather(up_w, "tp", axis=2, tiled=True)[0]
    down_piece = lax.all_gather(down_w, "tp", axis=2, tiled=True)[0]
    produced = expert_rows(slot_rows, gate_piece, up_piece, down_piece)
    results = produced.astype(BF16).reshape(sources, items, width)
    answered = lax.all_to_all(results, sp, split_axis=0, concat_axis=0, tiled=True)
    flat_answers = answered.reshape(experts_all * capacity, normed.shape[1])
    per_route = jnp.einsum("rks,sd->rkd", selector, flat_answers, preferred_element_type=F32)
    return jnp.sum(per_route * weight[:, :, None], axis=1)


def body(
    residual,
    query_values,
    forget_preact,
    value_written,
    output_gate_preact,
    forget_margin,
    sudden_decay,
    head_norm_gain,
    output_weight_matrix,
    mixer_norm_gain,
    feedforward_gain,
    routed_expert_index,
    routed_expert_weight,
    expert_gate_matrix,
    expert_up_matrix,
    expert_down_matrix,
    common_gate_matrix,
    common_up_matrix,
    common_down_matrix,
    final_norm_gain,
    *,
    sp,
):
    tokens, channels = query_values.shape
    rows = residual.shape[0]
    peers = lax.axis_size("tp")
    paired = len(sp) == 2
    if paired:
        outer, inner = sp
        ring = (inner, "tp")
        forward, backward, partner = ring_hops(lax.axis_size(inner), peers)
        upper, lower = pack_call(expert_gate_matrix, expert_up_matrix, expert_down_matrix)
        hops = {"long": ([upper], [lower]), "short": ([lower], [upper])}

        def hop(kind):
            for perm, chain in zip((forward, backward), hops[kind]):
                chain.append(lax.ppermute(chain[-1], ring, perm))

        hop("long")
        hop("short")
        level = lax.axis_index("tp") // 2
        size = peers
        place = jnp.where(lax.axis_index(inner) == 0, level, size - 1 - level)
        origin = [place, place]
        for k in range(1, size // 2):
            origin += [place - k, place - k, place + k, place + k]
        origin += [place + size // 2] * 2
        which = ((jnp.stack(origin) % size) >= size // 2).astype(jnp.int32)
        experts_all = lax.axis_size(outer) * lax.axis_size(inner)
        share = jnp.stack(
            [
                jnp.sum(jnp.where(routed_expert_index == e, routed_expert_weight, 0.0), axis=1)
                for e in range(experts_all)
            ]
        )
        pair = lax.axis_size(inner)
        swap = [(0, 1), (1, 0)]
        here = lax.axis_index(outer) == 0
        filler = jnp.zeros((8 - pair, rows), F32)
        own_share = jnp.concatenate([jnp.where(here, share[:pair], share[pair:]), filler])
        far_share = jnp.concatenate([jnp.where(here, share[pair:], share[:pair]), filler])
        far_share = lax.ppermute(far_share, outer, swap)

    local, lifted, final = scan_call(
        query_values, forget_preact, value_written, forget_margin, sudden_decay
    )
    mine = lax.axis_index(sp)
    if paired:
        others = [
            lax.ppermute(final, sp, [(i, i ^ other) for i in range(4)]) for other in (1, 2, 3)
        ]
        pieces = jnp.stack([final] + others)
        order = mine ^ jnp.arange(4)
        hop("long")
        hop("short")
    else:
        pieces = lax.all_gather(final, sp)
        order = jnp.arange(pieces.shape[0])
    mine = jnp.concatenate([mine.reshape(1), order])
    gain = jnp.tile(head_norm_gain, channels // HEAD_CHANNELS).reshape(1, channels)
    mixed = gate_call(mine, local, lifted, output_gate_preact, pieces, gain)
    mixed = lax.all_to_all(
        mixed.reshape(peers, tokens // peers, channels), "tp", split_axis=0, concat_axis=0, tiled=True
    )
    if paired:
        hop("long")
        hop("short")
        held = []

        def hold(slot, start, array):
            held.append((array, slot, start))
            held.append((lax.ppermute(array, "tp", partner), slot + 1, start))

        def hold_hop(k):
            hold(4 * k - 2, 0, long_a[k])
            hold(4 * k - 2, half, short_a[k])
            hold(4 * k, 0, short_b[k])
            hold(4 * k, half, long_b[k])

        half = upper.shape[0]
        (long_a, long_b), (short_a, short_b) = hops["long"], hops["short"]
        hold(0, 0, upper)
        hold(0, half, lower)
        hold_hop(1)
        mixed, which, own_share, far_share, early = lax.optimization_barrier(
            (mixed, which, own_share, far_share, [array for array, _, _ in held])
        )
        held = [(array, slot, start) for array, (_, slot, start) in zip(early, held)]
    if channels % 128 == 0:
        stream, normed, shared = project_call(
            mixed,
            output_weight_matrix,
            residual,
            mixer_norm_gain,
            feedforward_gain,
            (common_gate_matrix, common_up_matrix, common_down_matrix),
        )
    else:
        mixed = mixed.transpose(1, 0, 2).reshape(rows, peers * channels)
        projected = jnp.dot(mixed, output_weight_matrix, preferred_element_type=F32).astype(BF16)
        stream = (residual.astype(F32) + rms_scale(projected.astype(F32)) * mixer_norm_gain).astype(BF16)
        normed = (rms_scale(stream.astype(F32)) * feedforward_gain).astype(BF16)
        shared = shared_expert(normed, common_gate_matrix, common_up_matrix, common_down_matrix)
    if not paired:
        routed = routed_by_slots(
            normed,
            routed_expert_index,
            routed_expert_weight,
            expert_gate_matrix,
            expert_up_matrix,
            expert_down_matrix,
            sp,
        )
        layer_out = stream.astype(F32) + rms_scale(shared + routed) * final_norm_gain
        return layer_out.astype(BF16)
    first = 3 * rows // 8
    far_first = lax.ppermute(normed[:first], outer, swap)
    far_rest = lax.ppermute(normed[first:], outer, swap)
    hop("long")

    hold_hop(2)
    hold_hop(3)
    hold(14, 0, long_a[4])
    hold(14, half, long_b[4])
    (partial,) = expert_call(which, far_first, far_share, held, None, (first,), BF16)
    answers = [lax.ppermute(partial, outer, swap)]
    far_rest, _ = lax.optimization_barrier((far_rest, partial))
    sizes = (rows - 2 * first, first)
    partials = expert_call(which, far_rest, far_share, held, None, sizes, BF16, first)
    answers += [lax.ppermute(partial, outer, swap) for partial in partials]
    own_rows, _ = lax.optimization_barrier((normed, partials[1]))
    (base,) = expert_call(which, own_rows, own_share, held, shared, (rows,), F32)
    starts = (0, first, first + sizes[0])
    layer_out = None
    for chosen in ((0, 2), (1,)):
        layer_out = combine_call(
            layer_out,
            stream,
            base,
            [answers[c] for c in chosen],
            final_norm_gain,
            [starts[c] for c in chosen],
        )
    return layer_out


def solution(mesh):
    sp_size, tp_size = mesh.shape["sp"], mesh.shape["tp"]
    if sp_size == 4:
        sp = ("far", "near")
        mesh = Mesh(mesh.devices.reshape(2, 2, tp_size), sp + ("tp",))
    else:
        sp = ("sp",)
    every = P(sp + ("tp",), None)
    split = P(sp, "tp")
    shard = P(sp, None, "tp")
    placed = (
        every,
        split,
        split,
        split,
        split,
        P("tp"),
        P("tp", sp),
        P(),
        P(),
        P(),
        P(),
        every,
        every,
        shard,
        shard,
        shard,
        P(),
        P(),
        P(),
        P(),
    )

    def step(*arrays):
        return body(*arrays, sp=sp)

    return jax.shard_map(step, mesh=mesh, in_specs=placed, out_specs=every, check_vma=False)
```

```python
import functools

import jax
import jax.numpy as jnp
from jax import lax
from jax.experimental import pallas as pl
from jax.experimental.pallas import tpu as pltpu
from jax.sharding import Mesh, PartitionSpec as P


HEAD_CHANNELS = 64
BLOCK = 64
EPS = 1e-06
TOP_PRECISION = lax.Precision.HIGHEST
F32 = jnp.float32
BF16 = jnp.bfloat16

LANES_LANES = (((1,), (1,)), ((), ()))
ROWS_ROWS = (((0,), (0,)), ((), ()))


def rms_scale(values):
    return values * lax.rsqrt(jnp.mean(values * values, axis=-1, keepdims=True) + EPS)


def mm(a, b, dims=(((1,), (0,)), ((), ()))):
    return lax.dot_general(a, b, dims, preferred_element_type=F32)


def halves(value):
    top = value.astype(BF16)
    return top, (value - top.astype(F32)).astype(BF16)


def fine_mm(a, b):
    a_top, a_rest = a
    b_top, b_rest = b
    return mm(
        jnp.concatenate([a_top, a_rest, a_top], axis=1),
        jnp.concatenate([b_top, b_top, b_rest], axis=1),
        LANES_LANES,
    )


def scan_kernel(
    q_ref, f_ref, v_ref, margin_ref, sudden_ref, local_ref, lifted_ref, final_ref, state_ref, total_ref
):
    step = pl.program_id(0)
    span, channels = q_ref.shape
    heads = channels // HEAD_CHANNELS

    @pl.when(step == 0)
    def _():
        state_ref[...] = jnp.zeros_like(state_ref)
        total_ref[...] = jnp.zeros_like(total_ref)

    lane = lax.broadcasted_iota(jnp.int32, (BLOCK, channels), 1) // HEAD_CHANNELS

    def per_head(block):
        if heads == 1:
            return block
        return jnp.concatenate(
            [jnp.where(lane == h, block, jnp.zeros_like(block)) for h in range(heads)], axis=0
        )

    rows = lax.broadcasted_iota(jnp.int32, (BLOCK, heads * BLOCK), 0)
    cols = lax.broadcasted_iota(jnp.int32, (BLOCK, heads * BLOCK), 1) % BLOCK
    lower = rows >= cols
    sum_rows = lax.broadcasted_iota(jnp.int32, (BLOCK, 3 * BLOCK), 0)
    sum_cols = lax.broadcasted_iota(jnp.int32, (BLOCK, 3 * BLOCK), 1) % BLOCK
    summing = (sum_rows >= sum_cols).astype(F32).astype(BF16)
    own_head = (
        lax.broadcasted_iota(jnp.int32, (channels, channels), 0) // HEAD_CHANNELS
        == lax.broadcasted_iota(jnp.int32, (channels, channels), 1) // HEAD_CHANNELS
    )
    margin = margin_ref[...]
    sudden = sudden_ref[...]
    sudden = jnp.concatenate([sudden, jnp.zeros((8 - heads, span), F32)], axis=0).T
    state = state_ref[...]
    total = total_ref[...]
    for j in range(span // BLOCK):
        at = pl.ds(j * BLOCK, BLOCK)
        strength = margin * jax.nn.sigmoid(-f_ref[at, :].astype(F32))
        extra = sudden[j * BLOCK : (j + 1) * BLOCK]
        jump = jnp.broadcast_to(extra[:, 0:1], (BLOCK, channels))
        for h in range(1, heads):
            jump = jnp.where(lane == h, jnp.broadcast_to(extra[:, h : h + 1], (BLOCK, channels)), jump)
        keep = jnp.log1p(-strength) + jump
        top = keep.astype(BF16)
        rest = keep - top.astype(F32)
        second = rest.astype(BF16)
        third = (rest - second.astype(F32)).astype(BF16)
        running = mm(summing, jnp.concatenate([top, second, third], axis=0))
        middle = running[BLOCK // 2 - 1 : BLOCK // 2]
        closing = running[BLOCK - 1 : BLOCK]
        scaled_q = q_ref[at, :].astype(F32) * jnp.exp(running - middle)
        scaled_k = strength * jnp.exp(middle - running)
        values = v_ref[at, :]
        k_top, k_rest = halves(scaled_k)
        scores = fine_mm(halves(scaled_q), (per_head(k_top), per_head(k_rest)))
        score_top, score_rest = halves(jnp.where(lower, scores, 0.0))
        spread = per_head(values)
        lifted = scaled_q * jnp.exp(middle)
        local_ref[at, :] = mm(
            jnp.concatenate([score_top, score_rest], axis=1), jnp.concatenate([spread, spread], axis=0)
        ) + fine_mm(halves(lifted), halves(state))
        lifted_ref[at, :] = lifted * jnp.exp(total)
        closed_k = jnp.concatenate(halves(scaled_k * jnp.exp(closing - middle)), axis=0)
        added = mm(jnp.concatenate([values, values], axis=0), closed_k, ROWS_ROWS)
        state = state * jnp.exp(closing) + jnp.where(own_head, added, 0.0)
        total = total + closing
    state_ref[...] = state
    total_ref[...] = total
    final_ref[0:channels, :] = state
    final_ref[channels:, :] = jnp.broadcast_to(jnp.exp(total), (8, channels))


def scan_call(q, f, v, margin, sudden):
    tokens, channels = q.shape
    heads = channels // HEAD_CHANNELS
    span = min(tokens, 512)
    block = pl.BlockSpec((span, channels), lambda i: (i, 0))
    return pl.pallas_call(
        scan_kernel,
        grid=(tokens // span,),
        in_specs=[
            block,
            block,
            block,
            pl.BlockSpec((1, channels), lambda i: (0, 0)),
            pl.BlockSpec((heads, span), lambda i: (0, i)),
        ],
        out_specs=[block, block, pl.BlockSpec((channels + 8, channels), lambda i: (0, 0))],
        out_shape=[
            jax.ShapeDtypeStruct((tokens, channels), F32),
            jax.ShapeDtypeStruct((tokens, channels), F32),
            jax.ShapeDtypeStruct((channels + 8, channels), F32),
        ],
        scratch_shapes=[pltpu.VMEM((channels, channels), F32), pltpu.VMEM((1, channels), F32)],
        compiler_params=pltpu.CompilerParams(dimension_semantics=("arbitrary",)),
        cost_estimate=pl.CostEstimate(
            flops=tokens * channels * 2000, bytes_accessed=tokens * channels * 14, transcendentals=0
        ),
        name="scan",
    )(q, f, v, margin.reshape(1, channels), sudden)


def gate_kernel(mine_ref, local_ref, lifted_ref, open_ref, pieces_ref, gain_ref, mixed_ref):
    _, channels = local_ref.shape
    mine = mine_ref[0]
    incoming = jnp.zeros((channels, channels), F32)
    for j in range(pieces_ref.shape[0] - 1):
        at = mine_ref[1 + j]
        longer = incoming * pieces_ref[at, channels : channels + 1, :] + pieces_ref[at, 0:channels, :]
        incoming = jnp.where(j < mine, longer, incoming)
    heads_out = local_ref[...] + fine_mm(halves(lifted_ref[...]), halves(incoming))
    own_head = (
        lax.broadcasted_iota(jnp.int32, (channels, channels), 0) // HEAD_CHANNELS
        == lax.broadcasted_iota(jnp.int32, (channels, channels), 1) // HEAD_CHANNELS
    )
    averaging = jnp.where(own_head, 1.0 / HEAD_CHANNELS, 0.0).astype(BF16)
    square = heads_out * heads_out
    top = square.astype(BF16)
    rest = (square - top.astype(F32)).astype(BF16)
    mean = mm(top, averaging) + mm(rest, averaging)
    opening = jax.nn.sigmoid(open_ref[...].astype(F32))
    mixed_ref[...] = (heads_out * lax.rsqrt(mean + EPS) * gain_ref[...] * opening).astype(BF16)


def gate_call(mine, local, lifted, opening, pieces, gain):
    tokens, channels = local.shape
    span = min(tokens, 1024)
    block = pl.BlockSpec((span, channels), lambda i: (i, 0))
    return pl.pallas_call(
        gate_kernel,
        grid=(tokens // span,),
        in_specs=[
            pl.BlockSpec(memory_space=pltpu.SMEM),
            block,
            block,
            block,
            pl.BlockSpec(pieces.shape, lambda i: (0, 0, 0)),
            pl.BlockSpec((1, channels), lambda i: (0, 0)),
        ],
        out_specs=block,
        out_shape=jax.ShapeDtypeStruct((tokens, channels), BF16),
        compiler_params=pltpu.CompilerParams(dimension_semantics=("arbitrary",)),
        cost_estimate=pl.CostEstimate(
            flops=tokens * channels * 800, bytes_accessed=tokens * channels * 10, transcendentals=0
        ),
        name="gate",
    )(mine, local, lifted, opening, pieces, gain)


def project_kernel(
    mixed_ref,
    weight_ref,
    residual_ref,
    mixer_ref,
    gain_ref,
    gate_ref,
    up_ref,
    down_ref,
    stream_ref,
    normed_ref,
    shared_ref,
):
    mixed = jnp.concatenate([mixed_ref[j] for j in range(mixed_ref.shape[0])], axis=1)
    projected = mm(mixed, weight_ref[...]).astype(BF16).astype(F32)
    stream = (residual_ref[...].astype(F32) + rms_scale(projected) * mixer_ref[...]).astype(BF16)
    stream_ref[...] = stream
    normed = (rms_scale(stream.astype(F32)) * gain_ref[...]).astype(BF16)
    normed_ref[...] = normed
    gate = mm(normed, gate_ref[...])
    hidden = (gate * jax.nn.sigmoid(gate) * mm(normed, up_ref[...])).astype(BF16)
    shared_ref[...] = mm(hidden, down_ref[...])


def project_call(mixed, weight, residual, mixer_gain, gain, shared_weights):
    sources, rows, channels = mixed.shape
    width = weight.shape[1]
    span = min(rows, 256)
    block = pl.BlockSpec((span, width), lambda i: (i, 0))

    def whole(array):
        return pl.BlockSpec(array.shape, lambda i: (0, 0))

    vectors = [mixer_gain.reshape(1, width), gain.reshape(1, width)]
    hidden = shared_weights[0].shape[1]
    return pl.pallas_call(
        project_kernel,
        grid=(rows // span,),
        in_specs=[pl.BlockSpec((sources, span, channels), lambda i: (0, i, 0)), whole(weight), block]
        + [whole(array) for array in vectors + list(shared_weights)],
        out_specs=[block, block, block],
        out_shape=[
            jax.ShapeDtypeStruct((rows, width), BF16),
            jax.ShapeDtypeStruct((rows, width), BF16),
            jax.ShapeDtypeStruct((rows, width), F32),
        ],
        compiler_params=pltpu.CompilerParams(
            dimension_semantics=("arbitrary",), vmem_limit_bytes=48 * 1024 * 1024
        ),
        cost_estimate=pl.CostEstimate(
            flops=2 * rows * width * (weight.shape[0] + 3 * hidden),
            bytes_accessed=2 * weight.size + 12 * rows * width,
            transcendentals=0,
        ),
        name="project",
    )(mixed, weight, residual, *vectors, *shared_weights)


def pack_kernel(gate_ref, up_ref, down_ref, upper_ref, lower_ref):
    width, units = gate_ref.shape[1:]
    half = upper_ref.shape[0]
    upper_ref[:, 0:units] = gate_ref[0, 0:half, :]
    upper_ref[:, units:] = up_ref[0, 0:half, :]
    lower_ref[0 : width - half, 0:units] = gate_ref[0, half:, :]
    lower_ref[0 : width - half, units:] = up_ref[0, half:, :]
    for j in range(width // (2 * units)):
        turned = down_ref[0, j * 2 * units : (j + 1) * 2 * units, :].T
        lower_ref[width - half + j * units : width - half + (j + 1) * units, :] = turned


def pack_call(gate, up, down):
    _, width, units = gate.shape
    return pl.pallas_call(
        pack_kernel,
        out_shape=[jax.ShapeDtypeStruct((3 * width // 4, 2 * units), gate.dtype)] * 2,
        cost_estimate=pl.CostEstimate(flops=0, bytes_accessed=12 * width * units, transcendentals=0),
        name="pack",
    )(gate, up, down)


def expert_kernel(*refs, based, sources, skip):
    which_ref, rows_ref, share_ref = refs[:3]
    piece_refs = refs[3 + based : 3 + based + len(sources)]
    out_refs = refs[3 + based + len(sources) : -4]
    held_ref, sum_ref, wide_ref, sems = refs[-4:]
    width = rows_ref.shape[1]
    pieces, _, double = held_ref.shape
    units = double // 2
    for ref, (slot, start) in zip(piece_refs, sources):
        into = held_ref.at[slot, start : start + ref.shape[0]]
        pltpu.make_async_copy(ref, into, sems.at[slot]).start()
    sum_ref[...] = jnp.zeros_like(sum_ref)
    share = share_ref[...].T[skip : skip + rows_ref.shape[0]]
    for e in range(wide_ref.shape[0]):
        wide_ref[e] = jnp.broadcast_to(share[:, e : e + 1], wide_ref.shape[1:])

    for g in range(pieces // TOGETHER):
        slots = range(g * TOGETHER, (g + 1) * TOGETHER)
        for slot in slots:
            pltpu.make_async_copy(held_ref.at[slot], held_ref.at[slot], sems.at[slot]).wait()
        hidden = []
        for slot in slots:
            part = wide_ref[which_ref[slot]]
            both = mm(rows_ref[...], held_ref[slot, 0:width, :])
            gate, up = both[:, :units], both[:, units:]
            hidden.append((gate * jax.nn.sigmoid(gate) * up * part).astype(BF16))
        hidden = jnp.concatenate(hidden, axis=1)
        for c in range(width // double):
            at = slice(width + c * units, width + (c + 1) * units)
            down = jnp.concatenate([held_ref[slot, at, :] for slot in slots], axis=0)
            sum_ref[:, c * double : (c + 1) * double] += mm(hidden, down)
    start = 0
    for out_ref in out_refs:
        at = slice(start, start + out_ref.shape[0])
        total = sum_ref[at, :] + refs[3][at, :] if based else sum_ref[at, :]
        out_ref[...] = total.astype(out_ref.dtype)
        start += out_ref.shape[0]


TOGETHER = 2


def expert_call(which, rows, share, held, base, sizes, kind, skip=0):
    count, width = rows.shape
    arrays = [array for array, _, _ in held]
    sources = [(slot, start) for _, slot, start in held]
    double = arrays[0].shape[1]
    depth = width + width // 2
    pieces = 1 + max(slot for slot, _ in sources)
    specs = [pl.BlockSpec(memory_space=pltpu.SMEM)] + [pl.BlockSpec(memory_space=pltpu.VMEM)] * 2
    operands = [which, rows, share]
    if base is not None:
        specs.append(pl.BlockSpec(memory_space=pltpu.VMEM))
        operands.append(base)
    specs += [pl.BlockSpec(memory_space=pltpu.HBM)] * len(arrays)
    return pl.pallas_call(
        functools.partial(expert_kernel, based=base is not None, sources=sources, skip=skip),
        in_specs=specs,
        out_specs=[pl.BlockSpec(memory_space=pltpu.VMEM)] * len(sizes),
        out_shape=[jax.ShapeDtypeStruct((size, width), kind) for size in sizes],
        scratch_shapes=[
            pltpu.VMEM((pieces, depth, double), BF16),
            pltpu.VMEM((count, width), F32),
            pltpu.VMEM((2, count, double // 2), F32),
            pltpu.SemaphoreType.DMA((pieces,)),
        ],
        compiler_params=pltpu.CompilerParams(vmem_limit_bytes=60 * 1024 * 1024),
        cost_estimate=pl.CostEstimate(
            flops=2 * count * pieces * depth * double,
            bytes_accessed=2 * pieces * depth * double,
            transcendentals=0,
        ),
    )(*operands, *arrays)


def ring_hops(columns, peers):
    long = peers // 2
    size = columns * long

    def device(r, core):
        column, level = (0, r) if r < long else (1, size - 1 - r)
        return column * peers + level * 2 + core

    def shift(by):
        return [(device(r, c), device((r + by) % size, c)) for r in range(size) for c in (0, 1)]

    swap = [(z * 2 + c, z * 2 + 1 - c) for z in range(long) for c in (0, 1)]
    return shift(1), shift(-1), swap


def combine_kernel(*refs, counts, followed):
    stream_ref, base_ref = refs[followed : followed + 2]
    answer_refs = refs[followed + 2 : -2]
    gain_ref, out_ref = refs[-2:]
    answer = answer_refs[0][...]
    if len(counts) == 2:
        answer = jnp.where(pl.program_id(0) < counts[0], answer, answer_refs[1][...])
    summed = base_ref[...] + answer.astype(F32)
    out_ref[...] = (stream_ref[...].astype(F32) + rms_scale(summed) * gain_ref[...]).astype(BF16)


def combine_call(so_far, stream, base, answers, gain, starts):
    rows, width = stream.shape
    span = min(answers[0].shape[0], 64)
    counts = [answer.shape[0] // span for answer in answers]
    skips = [start // span for start in starts]

    def place(i):
        if len(counts) == 1:
            return skips[0] + i, 0
        return jnp.where(i < counts[0], skips[0] + i, skips[1] + i - counts[0]), 0

    places = [
        lambda i: (jnp.minimum(i, counts[0] - 1), 0),
        lambda i: (jnp.maximum(i - counts[0], 0), 0),
    ]
    block = pl.BlockSpec((span, width), place)
    specs = [block, block] + [pl.BlockSpec((span, width), at) for at in places[: len(counts)]]
    specs.append(pl.BlockSpec((1, width), lambda i: (0, 0)))
    operands = [stream, base, *answers, gain.reshape(1, width)]
    aliases = {}
    if so_far is not None:
        specs.insert(0, pl.BlockSpec(memory_space=pl.ANY))
        operands.insert(0, so_far)
        aliases = {0: 0}
    return pl.pallas_call(
        functools.partial(combine_kernel, counts=counts, followed=int(so_far is not None)),
        grid=(sum(counts),),
        in_specs=specs,
        out_specs=block,
        out_shape=jax.ShapeDtypeStruct((rows, width), BF16),
        input_output_aliases=aliases,
        compiler_params=pltpu.CompilerParams(dimension_semantics=("arbitrary",)),
        cost_estimate=pl.CostEstimate(
            flops=sum(counts) * span * width,
            bytes_accessed=10 * sum(counts) * span * width,
            transcendentals=0,
        ),
    )(*operands)


def shared_expert(normed, gate_w, up_w, down_w):
    hidden = (
        jax.nn.silu(jnp.dot(normed, gate_w, preferred_element_type=F32))
        * jnp.dot(normed, up_w, preferred_element_type=F32)
    ).astype(BF16)
    return jnp.dot(hidden, down_w, preferred_element_type=F32)


def expert_rows(slot_rows, gate_w, up_w, down_w):
    hidden = (
        jax.nn.silu(jnp.dot(slot_rows, gate_w, preferred_element_type=F32))
        * jnp.dot(slot_rows, up_w, preferred_element_type=F32)
    ).astype(BF16)
    return lax.dot_general(hidden, down_w, LANES_LANES, preferred_element_type=F32)


def routed_by_slots(normed, index, weight, gate_w, up_w, down_w, sp):
    rows_here, routes_each = index.shape
    experts_all = lax.axis_size(sp)
    capacity = 3 * rows_here * routes_each // (2 * experts_all)
    numbers = jnp.arange(experts_all, dtype=jnp.int32)
    matches = (index[:, :, None] == numbers).astype(F32)
    hits = jnp.sum(matches, axis=1)
    strictly_lower = jnp.tril(jnp.ones((rows_here, rows_here), F32), -1)
    before_hits = jnp.dot(strictly_lower, hits, precision=TOP_PRECISION)
    slots = jnp.sum(before_hits[:, None, :] * matches, axis=2).astype(jnp.int32)
    targets = index * capacity + slots
    slot_numbers = jnp.arange(experts_all * capacity, dtype=jnp.int32)
    selector = (targets[:, :, None] == slot_numbers).astype(BF16)
    outgoing = jnp.einsum("rks,rd->sd", selector, normed, preferred_element_type=F32)
    outgoing = outgoing.astype(BF16).reshape(experts_all, capacity, normed.shape[1])
    arrived = lax.all_to_all(outgoing, sp, split_axis=0, concat_axis=0, tiled=True)
    sources, items, width = arrived.shape
    slot_rows = arrived.reshape(sources * items, width)
    gate_piece = lax.all_gather(gate_w, "tp", axis=2, tiled=True)[0]
    up_piece = lax.all_gather(up_w, "tp", axis=2, tiled=True)[0]
    down_piece = lax.all_gather(down_w, "tp", axis=2, tiled=True)[0]
    produced = expert_rows(slot_rows, gate_piece, up_piece, down_piece)
    results = produced.astype(BF16).reshape(sources, items, width)
    answered = lax.all_to_all(results, sp, split_axis=0, concat_axis=0, tiled=True)
    flat_answers = answered.reshape(experts_all * capacity, normed.shape[1])
    per_route = jnp.einsum("rks,sd->rkd", selector, flat_answers, preferred_element_type=F32)
    return jnp.sum(per_route * weight[:, :, None], axis=1)


def body(
    residual,
    query_values,
    forget_preact,
    value_written,
    output_gate_preact,
    forget_margin,
    sudden_decay,
    head_norm_gain,
    output_weight_matrix,
    mixer_norm_gain,
    feedforward_gain,
    routed_expert_index,
    routed_expert_weight,
    expert_gate_matrix,
    expert_up_matrix,
    expert_down_matrix,
    common_gate_matrix,
    common_up_matrix,
    common_down_matrix,
    final_norm_gain,
    *,
    sp,
):
    tokens, channels = query_values.shape
    rows = residual.shape[0]
    peers = lax.axis_size("tp")
    paired = len(sp) == 2
    if paired:
        outer, inner = sp
        ring = (inner, "tp")
        forward, backward, partner = ring_hops(lax.axis_size(inner), peers)
        upper, lower = pack_call(expert_gate_matrix, expert_up_matrix, expert_down_matrix)
        hops = {"long": ([upper], [lower]), "short": ([lower], [upper])}

        def hop(kind):
            for perm, chain in zip((forward, backward), hops[kind]):
                chain.append(lax.ppermute(chain[-1], ring, perm))

        hop("long")
        hop("short")
        level = lax.axis_index("tp") // 2
        size = peers
        place = jnp.where(lax.axis_index(inner) == 0, level, size - 1 - level)
        origin = [place, place]
        for k in range(1, size // 2):
            origin += [place - k, place - k, place + k, place + k]
        origin += [place + size // 2] * 2
        which = ((jnp.stack(origin) % size) >= size // 2).astype(jnp.int32)
        experts_all = lax.axis_size(outer) * lax.axis_size(inner)
        share = jnp.stack(
            [
                jnp.sum(jnp.where(routed_expert_index == e, routed_expert_weight, 0.0), axis=1)
                for e in range(experts_all)
            ]
        )
        pair = lax.axis_size(inner)
        swap = [(0, 1), (1, 0)]
        here = lax.axis_index(outer) == 0
        filler = jnp.zeros((8 - pair, rows), F32)
        own_share = jnp.concatenate([jnp.where(here, share[:pair], share[pair:]), filler])
        far_share = jnp.concatenate([jnp.where(here, share[pair:], share[:pair]), filler])
        far_share = lax.ppermute(far_share, outer, swap)

    local, lifted, final = scan_call(
        query_values, forget_preact, value_written, forget_margin, sudden_decay
    )
    mine = lax.axis_index(sp)
    if paired:
        others = [
            lax.ppermute(final, sp, [(i, i ^ other) for i in range(4)]) for other in (1, 2, 3)
        ]
        pieces = jnp.stack([final] + others)
        order = mine ^ jnp.arange(4)
        hop("long")
        hop("short")
    else:
        pieces = lax.all_gather(final, sp)
        order = jnp.arange(pieces.shape[0])
    mine = jnp.concatenate([mine.reshape(1), order])
    gain = jnp.tile(head_norm_gain, channels // HEAD_CHANNELS).reshape(1, channels)
    mixed = gate_call(mine, local, lifted, output_gate_preact, pieces, gain)
    mixed = lax.all_to_all(
        mixed.reshape(peers, tokens // peers, channels), "tp", split_axis=0, concat_axis=0, tiled=True
    )
    if paired:
        hop("long")
        hop("short")
        held = []

        def hold(slot, start, array):
            for j, one in enumerate((array, lax.ppermute(array, "tp", partner))):
                held.append((one, slot + j, start))

        def hold_hop(k):
            hold(4 * k - 2, 0, long_a[k])
            hold(4 * k - 2, half, short_a[k])
            hold(4 * k, 0, short_b[k])
            hold(4 * k, half, long_b[k])

        half = upper.shape[0]
        (long_a, long_b), (short_a, short_b) = hops["long"], hops["short"]
        hold(0, 0, upper)
        hold(0, half, lower)
        hold_hop(1)
        mixed, which, own_share, far_share, early = lax.optimization_barrier(
            (mixed, which, own_share, far_share, [array for array, _, _ in held])
        )
        held[:] = [(array, slot, start) for array, (_, slot, start) in zip(early, held)]
    if channels % 128 == 0:
        stream, normed, shared = project_call(
            mixed,
            output_weight_matrix,
            residual,
            mixer_norm_gain,
            feedforward_gain,
            (common_gate_matrix, common_up_matrix, common_down_matrix),
        )
    else:
        mixed = mixed.transpose(1, 0, 2).reshape(rows, peers * channels)
        projected = jnp.dot(mixed, output_weight_matrix, preferred_element_type=F32).astype(BF16)
        stream = (residual.astype(F32) + rms_scale(projected.astype(F32)) * mixer_norm_gain).astype(BF16)
        normed = (rms_scale(stream.astype(F32)) * feedforward_gain).astype(BF16)
        shared = shared_expert(normed, common_gate_matrix, common_up_matrix, common_down_matrix)
    if not paired:
        routed = routed_by_slots(
            normed,
            routed_expert_index,
            routed_expert_weight,
            expert_gate_matrix,
            expert_up_matrix,
            expert_down_matrix,
            sp,
        )
        layer_out = stream.astype(F32) + rms_scale(shared + routed) * final_norm_gain
        return layer_out.astype(BF16)
    first = 3 * rows // 8
    far_first = lax.ppermute(normed[:first], outer, swap)
    far_rest = lax.ppermute(normed[first:], outer, swap)
    hop("long")

    hold_hop(2)
    arrays = [array for array, _, _ in held]
    arrays, long_a[4], long_b[4] = lax.optimization_barrier((arrays, long_a[4], long_b[4]))
    held[:] = [(array, slot, start) for array, (_, slot, start) in zip(arrays, held)]
    hold_hop(3)
    hold(14, 0, long_a[4])
    hold(14, half, long_b[4])
    (partial,) = expert_call(which, far_first, far_share, held, None, (first,), BF16)
    answers = [lax.ppermute(partial, outer, swap)]
    far_rest, _ = lax.optimization_barrier((far_rest, partial))
    sizes = (rows - 2 * first, first)
    partials = expert_call(which, far_rest, far_share, held, None, sizes, BF16, first)
    answers += [lax.ppermute(partial, outer, swap) for partial in partials]
    own_rows, _ = lax.optimization_barrier((normed, partials[1]))
    (base,) = expert_call(which, own_rows, own_share, held, shared, (rows,), F32)
    starts = (0, first, first + sizes[0])
    layer_out = None
    for chosen in ((0, 2), (1,)):
        layer_out = combine_call(
            layer_out,
            stream,
            base,
            [answers[c] for c in chosen],
            final_norm_gain,
            [starts[c] for c in chosen],
        )
    return layer_out


def solution(mesh):
    sp_size, tp_size = mesh.shape["sp"], mesh.shape["tp"]
    if sp_size == 4:
        sp = ("far", "near")
        mesh = Mesh(mesh.devices.reshape(2, 2, tp_size), sp + ("tp",))
    else:
        sp = ("sp",)
    every = P(sp + ("tp",), None)
    split = P(sp, "tp")
    shard = P(sp, None, "tp")
    placed = (
        every,
        split,
        split,
        split,
        split,
        P("tp"),
        P("tp", sp),
        P(),
        P(),
        P(),
        P(),
        every,
        every,
        shard,
        shard,
        shard,
        P(),
        P(),
        P(),
        P(),
    )

    def step(*arrays):
        return body(*arrays, sp=sp)

    return jax.shard_map(step, mesh=mesh, in_specs=placed, out_specs=every, check_vma=False)
```
